256 devices in a mesh: grp: 2 (over y), fs: 32 (over z, core), tp: 4 (over x).
Axes of the slice: x: 4, y: 2, z: 16, core: 2. Of those that a mesh axis runs over, the one named last changes fastest.
The devices are a block of a 4x16x16 slice.
Arguments:
- tokens: bfloat16 [14336, 2048], P(('grp', 'fs'), 'tp'), parts along dimension 0, may hold values from -170 to 170
- routes: int32 [14336, 6], P(('grp', 'fs')), parts along dimension 0, may hold values from 0 to 63, all different within a row; in each aligned block of 224 rows (0 to 223, 224 to 447, ...) at most 28 rows name the same one
- route_weights: float32 [14336, 6], P(('grp', 'fs')), parts along dimension 0, may hold values from 0.2 to 1
- norm_gain: float32 [2048], P('fs'), may hold values from 0.1 to 1.9
- gate_experts: float32 [64, 2048, 512], P(None, 'fs', 'tp'), may hold values from -0.125 to 0.125
- up_experts: float32 [64, 2048, 512], P(None, 'fs', 'tp'), may hold values from -0.125 to 0.125
- down_experts: float32 [64, 512, 2048], P(None, 'fs', 'tp'), may hold values from -0.25 to 0.25
- shared_gate: float32 [2048, 512], P('fs', 'tp'), may hold values from -0.125 to 0.125
- shared_up: float32 [2048, 512], P('fs', 'tp'), may hold values from -0.125 to 0.125
- shared_down: float32 [512, 2048], P('fs', 'tp'), may hold values from -0.25 to 0.25
Outputs:
- mixed: bfloat16 [14336, 2048], P(('grp', 'fs'), 'tp'), parts along dimension 0
- gate_ready: bfloat16 [128, 2048, 512], P(('grp', 'fs'), None, 'tp'), parts along dimension 0
- up_ready: bfloat16 [128, 2048, 512], P(('grp', 'fs'), None, 'tp'), parts along dimension 0
- down_ready: bfloat16 [128, 512, 2048], P(('grp', 'fs'), 'tp'), parts along dimension 0
- shared_gate_ready: bfloat16 [4096, 512], P('grp', 'tp'), parts along dimension 0
- shared_up_ready: bfloat16 [4096, 512], P('grp', 'tp'), parts along dimension 0
- shared_down_ready: bfloat16 [1024, 2048], P(('grp', 'tp')), parts along dimension 0
The draws below stay inside these ranges and needn't reach their ends.
There are 2 independent parts, one for each index of `grp`. The reference program is written for one: setup_inputs(seed, part) draws one part's arguments, and reference() takes and returns one part's arrays. A program takes and returns all parts, laid end to end along the dimension named above; an argument that names none is the same for every part. Nothing has to cross between parts.
Inputs may be any that keep to these rules, and one draw needn't show every extreme that they name: `routes`: the 6 experts of a row differ; among the rows of one index of fs no expert is named more than 28 times, a bound that some block reaches.
All inputs are finite; a program needn't handle non-finite values.
Results may differ from the reference program's by a relative error of at most 0.013.
Values may be sent and summed in bfloat16 or wider, within the bound.
A program may use at most 128 MiB of HBM per device.

```python
import math
import jax
import jax.numpy as jnp
import numpy as np
from jax import lax

D = 2048
FF = 512
SF = 512
EXPERTS = 64
TOP_K = 6
TOK_DEV = 224
TOKENS = 7168
CAP = 28
N_TP = 4


def draw_tokens(key, part):
    key_rows = jax.random.fold_in(key, 11)
    key_cols = jax.random.fold_in(key, 12)
    key_base = jax.random.fold_in(key, 13)
    row_scale = jnp.exp(jax.random.uniform(key_rows, (TOKENS, 1), jnp.float32, 0.0, math.log(10.0)))
    col_scale = jnp.exp(jax.random.uniform(key_cols, (1, D), jnp.float32, 0.0, math.log(10.0)))
    base = jnp.clip(jax.random.normal(key_base, (TOKENS, D), jnp.float32), -5.0, 5.0)
    return (base * row_scale * col_scale / 3.0).astype(jnp.bfloat16)


def block_scale(own_key, dims, cuts, low, top_value):
    def one(dim, blocks):
        steps = jax.random.uniform(jax.random.fold_in(jax.random.fold_in(own_key, 6), dim), (blocks,), jnp.float32, low / len(cuts), top_value / len(cuts))
        return jnp.repeat(jnp.exp(steps), dims[dim] // blocks).reshape((-1,) + (1,) * (len(dims) - dim - 1))

    gain = one(*cuts[0])
    for cut in cuts[1:]:
        gain = gain * one(*cut)
    return gain


def shared_out(rng, own, number, rows, amount, top, most, slope):
    order = jax.random.permutation(rng, amount)
    heavy_load, common = portions_of(amount, rows * top, most, slope, True), portions_of(amount, rows * top, most, slope, False)
    places = jnp.arange(amount)

    def named(lengths, turn):
        used = int((lengths > 0).sum())
        fixed = max(1, used // 4)
        passed = fixed + (places - fixed + turn * (used - fixed)) % max(1, amount - fixed)
        return jnp.zeros((amount,), jnp.int32).at[order[jnp.where(places < fixed, places, passed)]].set(jnp.asarray(lengths, jnp.int32))

    lengths = jnp.where(number % 4 == 0, named(heavy_load, number // 4), named(common, number - number // 4 - 1))
    mixed = jax.random.permutation(jax.random.fold_in(own, 3), amount)
    giver, receiver = mixed[0:amount // 2 * 2:2], mixed[1:amount // 2 * 2:2]
    room = jnp.minimum(lengths[giver] - 1, most - lengths[receiver]) // 2
    room = jnp.where((giver == order[0]) | (receiver == order[0]) | (lengths[receiver] == 0), 0, jnp.maximum(room, 0))
    passed = jax.random.randint(jax.random.fold_in(own, 4), (amount // 2,), 0, 1 << 20) % (room + 1)
    lengths = lengths.at[giver].add(-passed).at[receiver].add(passed)
    members = jnp.searchsorted(jnp.cumsum(lengths), jnp.arange(rows * top), side="right").astype(jnp.int32)
    grid = members.reshape(top, rows).T
    grid = grid[jax.random.permutation(jax.random.fold_in(own, 1), rows)]
    turn = jax.random.randint(jax.random.fold_in(own, 2), (rows, 1), 0, top)
    return jnp.take_along_axis(grid, (jnp.arange(top)[None, :] + turn) % top, axis=1)


def portions_of(amount, total, reach, skew, full):
    portions = [(1 << 20) // math.isqrt(rank ** skew) + 1 for rank in range(1, amount + 1)]
    largest = reach if full else min(reach, max(-(-total // amount), total * portions[0] // sum(portions)))
    least = 1 if total - largest >= amount - 1 else 0
    counts, spare = [largest] + [least] * (amount - 1), total - largest - least * (amount - 1)
    while spare > 0:
        movable = [i for i in range(1, amount) if counts[i] < largest] or [i for i in range(1, amount) if counts[i] < reach]
        pool, left = sum([portions[i] for i in movable]), spare
        for i in movable:
            addition = min(reach - counts[i], max(1, left * portions[i] // pool), spare)
            counts[i] = counts[i] + addition
            spare = spare - addition
    return np.array(counts)


def normal_values(stream_key, shape, scale, most, pieces=(), kind=jnp.bfloat16):
    factor_of = block_scale(stream_key, shape, pieces, -0.22, 0.18) if pieces else 1.0
    array = jax.random.normal(stream_key, shape, jnp.float32) * scale * factor_of
    return jnp.minimum(jnp.maximum(array, -most), most).astype(kind)


def setup_inputs(seed: int = 0, part: int = 0) -> dict:
    splits = jax.random.split(jax.random.key(seed), 11)
    part_splits = jax.random.split(jax.random.fold_in(splits[10], part), 11)
    tokens = draw_tokens(jax.random.fold_in(jax.random.fold_in(splits[10], part), 71), part)
    routes_keys = jax.random.split(jax.random.fold_in(part_splits[1], 1), TOKENS // TOK_DEV)
    routes_turns = jax.random.permutation(jax.random.fold_in(part_splits[1], 3), TOKENS // TOK_DEV)
    routes = jax.vmap(lambda own, number: shared_out(jax.random.fold_in(part_splits[1], 2), own, number, TOK_DEV, EXPERTS, TOP_K, CAP, 1))(routes_keys, routes_turns).reshape((TOKENS, TOP_K))
    route_weights = jnp.clip(jnp.exp(math.log(1.0) - 1.609438 * jax.random.uniform(part_splits[2], (TOKENS, TOP_K), jnp.float32) ** block_scale(part_splits[2], (TOKENS, TOP_K), ((0, 32),), -0.2, 0.2)), 0.2, 1.0)
    norm_gain = jnp.clip(1.0 + 0.18 * jax.random.normal(splits[3], (D,), jnp.float32), 0.1, 1.9)
    gate_experts = normal_values(splits[4], (EXPERTS, D, FF), D ** -0.5, 0.125, ((1, 32), (2, 4)), jnp.float32)
    up_experts = normal_values(splits[5], (EXPERTS, D, FF), D ** -0.5, 0.125, ((1, 32), (2, 4)), jnp.float32)
    down_experts = normal_values(splits[6], (EXPERTS, FF, D), FF ** -0.5, 0.25, ((1, 32), (2, 4)), jnp.float32)
    shared_gate = normal_values(splits[7], (D, SF), D ** -0.5, 0.125, ((0, 32), (1, 4)), jnp.float32)
    shared_up = normal_values(splits[8], (D, SF), D ** -0.5, 0.125, ((0, 32), (1, 4)), jnp.float32)
    shared_down = normal_values(splits[9], (SF, D), SF ** -0.5, 0.25, ((0, 32), (1, 4)), jnp.float32)
    return {"tokens": tokens, "routes": routes, "route_weights": route_weights, "norm_gain": norm_gain, "gate_experts": gate_experts, "up_experts": up_experts, "down_experts": down_experts, "shared_gate": shared_gate, "shared_up": shared_up, "shared_down": shared_down}


def grouped_product(active, weight):
    groups = N_TP
    span_cols = active.shape[1] // groups
    totals = jnp.zeros((active.shape[0], weight.shape[1]), jnp.float32)
    for section in range(groups):
        product = jnp.dot(active[:, section * span_cols:(section + 1) * span_cols], weight[section * span_cols:(section + 1) * span_cols], preferred_element_type=jnp.float32)
        rounded = lax.optimization_barrier(product.astype(jnp.bfloat16))
        totals = totals + rounded.astype(jnp.float32)
    return totals

def reference(tokens, routes, route_weights, norm_gain, gate_experts, up_experts, down_experts, shared_gate, shared_up, shared_down):
    gate_ready = (gate_experts * norm_gain[None, :, None]).astype(jnp.bfloat16)
    up_ready = (up_experts * norm_gain[None, :, None]).astype(jnp.bfloat16)
    down_ready = down_experts.astype(jnp.bfloat16)
    shared_gate_ready = (shared_gate * norm_gain[:, None]).astype(jnp.bfloat16)
    shared_up_ready = (shared_up * norm_gain[:, None]).astype(jnp.bfloat16)
    shared_down_ready = shared_down.astype(jnp.bfloat16)
    widened = tokens.astype(jnp.float32)
    normed = (widened * lax.rsqrt(lax.optimization_barrier(jnp.mean(widened * widened, axis=1, keepdims=True)) + 1e-06)).astype(jnp.bfloat16)
    shared_active = (jax.nn.silu(jnp.dot(normed, shared_gate_ready, preferred_element_type=jnp.float32)) * jnp.dot(normed, shared_up_ready, preferred_element_type=jnp.float32)).astype(jnp.bfloat16)
    shared_rows = grouped_product(shared_active, shared_down_ready)
    blocks = TOKENS // TOK_DEV
    pairs = TOK_DEV * TOP_K
    block_routes = routes.reshape(blocks, pairs)
    onehot = (block_routes[:, :, None] == jnp.arange(EXPERTS, dtype=jnp.int32)[None, None, :]).astype(jnp.int32)
    earlier = jnp.cumsum(onehot, axis=1) - onehot
    slot_index = lax.optimization_barrier(jnp.sum(earlier * onehot, axis=2)).astype(jnp.int32)
    target = block_routes * CAP + slot_index
    token_index = (jnp.arange(TOKENS * TOP_K, dtype=jnp.int32) // TOP_K).astype(jnp.int32)
    flat_target = (target + (jnp.arange(blocks, dtype=jnp.int32) * (EXPERTS * CAP))[:, None]).reshape(-1)
    source = jnp.full((blocks * EXPERTS * CAP,), -1, jnp.int32).at[flat_target].set(token_index)
    source = source.reshape(blocks, EXPERTS, CAP).transpose(1, 0, 2).reshape(EXPERTS, blocks * CAP)

    def expert_rows(operands):
        row_index, gate_one, up_one, down_one = operands
        present = row_index >= 0
        inputs = jnp.where(present[:, None], normed[jnp.maximum(row_index, 0)], jnp.zeros((), jnp.bfloat16))
        active = (jax.nn.silu(jnp.dot(inputs, gate_one, preferred_element_type=jnp.float32)) * jnp.dot(inputs, up_one, preferred_element_type=jnp.float32)).astype(jnp.bfloat16)
        return grouped_product(active, down_one).astype(jnp.bfloat16)
    results = lax.map(expert_rows, (source, gate_ready, up_ready, down_ready))
    flat_results = results.reshape(EXPERTS * blocks * CAP, D)
    block_of = (jnp.arange(TOKENS, dtype=jnp.int32) // TOK_DEV)[:, None]
    position = routes * (blocks * CAP) + block_of * CAP + slot_index.reshape(TOKENS, TOP_K)
    mixed = shared_rows
    for choice_k in range(TOP_K):
        mixed = mixed + flat_results[position[:, choice_k]].astype(jnp.float32) * route_weights[:, choice_k:choice_k + 1]
    return (mixed.astype(jnp.bfloat16), gate_ready, up_ready, down_ready, shared_gate_ready, shared_up_ready, shared_down_ready)
```

```python
import functools

import jax
import jax.numpy as jnp
from jax import lax
from jax.experimental import pallas as pl
from jax.experimental.pallas import tpu as pltpu
from jax.sharding import PartitionSpec as P

MESH = pl.DeviceIdType.MESH
BF = jnp.bfloat16
F32 = jnp.float32
META = 16
SLOTS = 32


def remote(src, dst, send_sem, recv_sem, **where):
    return pltpu.make_async_remote_copy(
        src_ref=src, dst_ref=dst, send_sem=send_sem, recv_sem=recv_sem, device_id=where, device_id_type=MESH
    )


def far_first(count):
    half = count // 2
    order = [half]
    for d in range(1, half):
        order += [half - d, half + d]
    return order + [0]


def places(chips, cols):
    g, f, t = lax.axis_index("grp"), lax.axis_index("fs"), lax.axis_index("tp")
    c = lax.rem(f, 2)
    z = lax.div(f, 2)
    up = lax.rem(z + 1, chips) * 2 + c
    down = lax.rem(z + chips - 1, chips) * 2 + c
    other = f + 1 - 2 * c
    par = lax.rem(g, 2)
    pair = g + 1 - 2 * par
    right, left = lax.rem(t + 1, cols), lax.rem(t + cols - 1, cols)
    return f, t, c, z, up, down, other, par, pair, right, left


def greet(peers):
    barrier = pltpu.get_barrier_semaphore()
    for peer in peers:
        pl.semaphore_signal(barrier, inc=1, device_id=peer, device_id_type=MESH)
    pl.semaphore_wait(barrier, len(peers))


def collect_kernel(
    chips, cols, toks, held, top, blk, gu, x, xs, gw, sg, su, sd, gu2,
    buf, tri, zs, zr, cs, cr, rs, rr, ls, lr, fs_, fr, ys, yr,
):
    f, t, c, z, up, down, other, par, pair, right, left = places(chips, cols)
    half = chips // 2
    order = far_first(chips)
    pos = {r: p for p, r in enumerate(order)}
    rows = blk.shape[0]
    cut = rows // 2
    width = 2 * SLOTS
    span = sg.shape[0] // (2 * chips)
    dspan = sd.shape[0] // (2 * chips)
    lanes = sg.shape[1]
    wide = tri.shape[0]
    greet([{"fs": up}, {"fs": down}, {"fs": other}, {"tp": right}, {"tp": left}, {"grp": pair}])
    sent = []

    def go(copy):
        copy.start()
        sent.append(copy)
        return copy

    plus, minus, sib = {}, {}, {}
    plus[1] = go(remote(blk, buf.at[chips - 1, c], zs.at[0, 0], zr.at[0, 0], fs=up))
    minus[1] = go(remote(blk, buf.at[1, c], zs.at[1, 0], zr.at[1, 0], fs=down))
    sib[0] = go(remote(blk, buf.at[0, c], cs.at[0], cr.at[0], fs=other))
    mine = blk.at[pl.ds(0, toks)]
    last = chips
    to_right, to_left, onward = {}, {}, {}
    to_right[last] = go(remote(mine, xs.at[t], rs.at[last], rr.at[last], tp=right))
    to_left[last] = go(remote(mine, xs.at[t], ls.at[last], lr.at[last], tp=left))
    swap = go(remote(gu, gu2, ys, yr, grp=pair))
    xs[t] = blk[0:toks]
    buf[0, c] = blk[...]
    tri[...] = jnp.where(
        lax.broadcasted_iota(jnp.int32, (wide, wide), 0) < lax.broadcasted_iota(jnp.int32, (wide, wide), 1), 1.0, 0.0
    ).astype(BF)

    def process(r):
        p = pos[r]

        @pl.loop(0, 2)
        def _(cc):
            meta = buf[r, cc, toks : toks + META, :].astype(F32)
            route, hi, lo = meta[0:top, 0:wide], meta[0:top, wide:], meta[top : 2 * top, 0:wide]
            named, his, los = [], [], []
            for j in range(held):
                hit = route == (f * held + j).astype(F32)
                named.append(jnp.sum(jnp.where(hit, 1.0, 0.0), axis=0, keepdims=True))
                his.append(jnp.sum(jnp.where(hit, hi, 0.0), axis=0, keepdims=True))
                los.append(jnp.sum(jnp.where(hit, lo, 0.0), axis=0, keepdims=True))
            stack = jnp.concatenate(named + [jnp.zeros((8 - held, wide), F32)], axis=0)
            rank = jnp.dot(stack.astype(BF), tri[...], preferred_element_type=F32)
            slot = lax.broadcasted_iota(jnp.int32, (SLOTS, wide), 0).astype(F32)
            picks, ghi, glo = [], [], []
            for j in range(held):
                pick = jnp.where(slot == rank[j : j + 1], 1.0, 0.0) * named[j]
                picks.append(pick)
                ghi.append(pick * his[j])
                glo.append(pick * los[j])
            chosen = jnp.concatenate(picks, axis=0).astype(BF)
            gw[p, cc] = jnp.concatenate(ghi + glo, axis=0).astype(BF)
            got = jnp.dot(chosen, buf[r, cc, 0:wide, :], preferred_element_type=F32).astype(BF)
            at = pl.multiple_of(p * width + cc * SLOTS, SLOTS)
            for j in range(held):
                x[t, j, pl.ds(at, SLOTS), :] = got[j * SLOTS : (j + 1) * SLOTS]
            owner = lax.rem(z + r, chips) * 2 + cc
            piece = buf[r, cc, toks + META : toks + META + span // 2, :]
            row = pl.multiple_of(owner * span, span)
            for h in range(2):
                there = pl.ds(pl.multiple_of(row + h * (span // 2), span // 2), span // 2)
                sg[there, :] = piece[:, 2 * h * lanes : (2 * h + 1) * lanes]
                su[there, :] = piece[:, (2 * h + 1) * lanes : (2 * h + 2) * lanes]
            sd[pl.ds(pl.multiple_of(owner * dspan, dspan), dspan), :] = buf[r, cc, toks + META + span // 2 :, :]

    def block(q, p):
        return x.at[q, :, pl.ds(p * width, width), :]

    def send(r):
        p = pos[r]
        to_right[p] = go(remote(block(t, p), block(t, p), rs.at[p], rr.at[p], tp=right))
        to_left[p] = go(remote(block(t, p), block(t, p), ls.at[p], lr.at[p], tp=left))

    def pass_on(p):
        to_right[p].wait_recv()
        to_left[p].wait_recv()
        source, target = (left, right) if p % 2 == 0 else (right, left)
        ref = xs.at[source] if p == last else block(source, p)
        onward[p] = go(remote(ref, ref, fs_.at[p], fr.at[p], tp=target))

    sib[0].wait_recv()
    process(0)
    send(0)
    waiting = [[last, pos[0]]]
    for d in range(1, half + 1):
        plus[d].wait_recv()
        if d < half:
            src, dst = buf.at[chips - d, c], buf.at[chips - d - 1, c]
            if d + 1 == half:
                src, dst = src.at[pl.ds(0, cut)], dst.at[pl.ds(0, cut)]
            plus[d + 1] = go(remote(src, dst, zs.at[0, d], zr.at[0, d], fs=up))
            here = buf.at[chips - d, c]
            sib[chips - d] = go(remote(here, here, cs.at[chips - d], cr.at[chips - d], fs=other))
        minus[d].wait_recv()
        if d < half:
            src, dst = buf.at[d, c], buf.at[d + 1, c]
            if d + 1 == half:
                src, dst = src.at[pl.ds(cut, cut)], dst.at[pl.ds(cut, cut)]
            minus[d + 1] = go(remote(src, dst, zs.at[1, d], zr.at[1, d], fs=down))
        here = buf.at[d, c]
        sib[d] = go(remote(here, here, cs.at[d], cr.at[d], fs=other))
        near = [chips - d, d] if d < half else [half]
        for r in near:
            sib[r].wait_recv()
            process(r)
        for r in near:
            send(r)
        waiting.append([pos[r] for r in near])
        if len(waiting) > 2:
            for p in waiting.pop(0):
                pass_on(p)
    for group in waiting:
        for p in group:
            pass_on(p)
    for p in onward:
        onward[p].wait_recv()
    swap.wait_recv()
    for copy in sent:
        copy.wait_send()


def layer_kernel(
    chips, cols, x, xs, gw, gu, gu2, sg, su, sd, dn, mixed, dn2, od, os,
    act, sact, y, own, ss, sr, ps, pr, ms, mr, rs, rr, ls, lr, fs_, fr, cs, cr, zs, zr, ws, wr, ys, yr,
):
    f, t, c, z, up, down, other, par, pair, right, left = places(chips, cols)
    half = chips // 2
    order = far_first(chips)
    pos = {r: p for p, r in enumerate(order)}
    toks, quarter = mixed.shape
    lanes = sg.shape[1]
    width = 2 * SLOTS
    parts = 4
    per = chips // parts
    tall = per * width
    across = [lax.rem(t + d, cols) for d in range(1, cols)]
    greet([{"fs": up}, {"fs": down}, {"fs": other}, {"grp": pair}] + [{"tp": a} for a in across])
    sent = []

    def go(copy):
        copy.start()
        sent.append(copy)
        return copy

    swap = go(remote(dn, dn2, ys, yr, grp=pair))
    own_lanes = pl.ds(pl.multiple_of(t * lanes, lanes), lanes)

    @pl.loop(0, parts)
    def _(i):
        at = pl.ds(pl.multiple_of(i * tall, tall), tall)
        for j, weights in ((par, gu), (1 - par, gu2)):
            both = jnp.zeros((tall, 2 * lanes), F32)
            for q in range(cols):
                both += jnp.dot(x[q, j, at, :], weights[q * quarter : (q + 1) * quarter, :], preferred_element_type=F32)
            act[j, at, own_lanes] = (jax.nn.silu(both[:, :lanes]) * both[:, lanes:]).astype(BF)

    to_right, to_left, onward = {}, {}, {}

    def piece(q, i):
        cols_of = pl.ds(pl.multiple_of(q * lanes, lanes), lanes)
        return sact.at[:, cols_of] if i == parts else act.at[:, pl.ds(i * tall, tall), cols_of]

    def send(i):
        to_right[i] = go(remote(piece(t, i), piece(t, i), rs.at[i], rr.at[i], tp=right))
        to_left[i] = go(remote(piece(t, i), piece(t, i), ls.at[i], lr.at[i], tp=left))

    def pass_on(i):
        to_right[i].wait_recv()
        to_left[i].wait_recv()
        source, target = (left, right) if i % 2 == 0 else (right, left)
        onward[i] = go(remote(piece(source, i), piece(source, i), fs_.at[i], fr.at[i], tp=target))

    for i in range(parts):
        send(i)
    sgate = jnp.zeros((toks, lanes), F32)
    sup = jnp.zeros((toks, lanes), F32)
    for q in range(cols):
        there = slice(q * quarter, (q + 1) * quarter)
        sgate += jnp.dot(xs[q], sg[there, :], preferred_element_type=F32)
        sup += jnp.dot(xs[q], su[there, :], preferred_element_type=F32)
    sact[:, own_lanes] = (jax.nn.silu(sgate) * sup).astype(BF)
    send(parts)
    placed = []

    def place(kind, source, target):
        home = pl.ds(pl.multiple_of(t * quarter, quarter), quarter)
        for k, a in enumerate(across):
            rows_of = pl.ds(pl.multiple_of(a * lanes, lanes), lanes)
            placed.append(go(remote(source.at[rows_of, :], target.at[:, home], ws.at[kind, k], wr.at[kind, k], tp=a)))
        target[:, home] = source[pl.ds(pl.multiple_of(t * lanes, lanes), lanes), :]

    pass_on(0)
    pass_on(1)
    swap.wait_recv()
    sibs = {}

    def chunk(i):
        onward[i].wait_recv()
        for j, weights in ((par, dn), (1 - par, dn2)):
            y[j] = jnp.dot(act[j, i * tall : (i + 1) * tall, :], weights[...], preferred_element_type=F32).astype(BF)

        def combine(p, u, cc):
            at = pl.ds(pl.multiple_of(u * width + cc * SLOTS, SLOTS), SLOTS)
            found = jnp.concatenate([y[0, at, :], y[1, at, :]], axis=0)
            twice = jnp.concatenate([found, found], axis=0)
            whole = lax.dot_general(gw[p, cc], twice, (((0,), (0,)), ((), ())), preferred_element_type=F32)
            return whole[0:toks]

        for u in range(per):
            p = i * per + u
            ss[p] = combine(p, u, 1 - c).astype(BF)
            own[p] = combine(p, u, c)
            sibs[p] = go(remote(ss.at[p], sr.at[p], cs.at[p], cr.at[p], fs=other))

    plus, minus = {}, {}
    cut = toks // 2

    def local(r):
        p = pos[r]
        sibs[p].wait_recv()
        return own[p] + sr[p].astype(F32)

    def step(k):
        if k == 0:
            both = local(half)
            ps[0, 0:cut] = both[0:cut].astype(BF)
            ms[0, cut:] = both[cut:].astype(BF)
            low, high = pl.ds(0, cut), pl.ds(cut, cut)
            plus[0] = go(remote(ps.at[0, low], pr.at[0, low], zs.at[0, 0], zr.at[0, 0], fs=up))
            minus[0] = go(remote(ms.at[0, high], mr.at[0, high], zs.at[1, 0], zr.at[1, 0], fs=down))
            return
        ahead, behind = local(half - k), local(half + k)
        plus[k - 1].wait_recv()
        if k == 1:
            ps[1, 0:cut] = (ahead[0:cut] + pr[0, 0:cut].astype(F32)).astype(BF)
            ps[1, cut:] = ahead[cut:].astype(BF)
        else:
            ps[k] = (ahead + pr[k - 1].astype(F32)).astype(BF)
        plus[k] = go(remote(ps.at[k], pr.at[k], zs.at[0, k], zr.at[0, k], fs=up))
        minus[k - 1].wait_recv()
        if k == 1:
            ms[1, 0:cut] = behind[0:cut].astype(BF)
            ms[1, cut:] = (behind[cut:] + mr[0, cut:].astype(F32)).astype(BF)
        else:
            ms[k] = (behind + mr[k - 1].astype(F32)).astype(BF)
        minus[k] = go(remote(ms.at[k], mr.at[k], zs.at[1, k], zr.at[1, k], fs=down))

    done = 0
    for i in range(parts):
        if i + 2 <= parts:
            pass_on(i + 2)
        chunk(i)
        if i == 0:
            place(0, dn, od.at[par])
            place(1, dn2, od.at[1 - par])
            place(2, sd, os)
        while done < half and max(pos[half - done], pos[(half + done) % chips]) < (i + 1) * per and done <= 2 * i:
            step(done)
            done += 1
    onward[parts].wait_recv()
    shared = jnp.dot(sact[...], sd[...], preferred_element_type=F32)
    while done < half:
        step(done)
        done += 1
    total = local(0) + shared
    plus[half - 1].wait_recv()
    minus[half - 1].wait_recv()
    total = total + pr[half - 1].astype(F32) + mr[half - 1].astype(F32)
    mixed[...] = total.astype(BF)
    for copy in placed:
        copy.wait_recv()
    for copy in sent:
        copy.wait_send()


VM = pl.BlockSpec(memory_space=pltpu.VMEM)


def shape(*dims, kind=BF):
    return jax.ShapeDtypeStruct(dims, kind)


def per_device(
    tokens, routes, route_weights, norm_gain, gate_experts, up_experts, down_experts, shared_gate, shared_up, shared_down
):
    fs_count, cols = lax.axis_size("fs"), lax.axis_size("tp")
    chips = fs_count // 2
    par = lax.rem(lax.axis_index("grp"), 2)
    experts, span, lanes = gate_experts.shape
    held = experts // fs_count
    toks, quarter = tokens.shape
    top = routes.shape[1]
    dspan = down_experts.shape[1]
    wide = quarter // 2

    def half_of(w):
        return lax.dynamic_index_in_dim(w.reshape(fs_count, held, *w.shape[1:]), par, 1, keepdims=False)

    gain = norm_gain[None, :, None]
    gu_cast = jnp.concatenate([half_of(gate_experts) * gain, half_of(up_experts) * gain], axis=2).astype(BF)
    gu = lax.all_to_all(gu_cast, "fs", 0, 0, tiled=True).reshape(fs_count * span, 2 * lanes)
    dn = lax.all_to_all(half_of(down_experts).astype(BF), "fs", 0, 0, tiled=True).reshape(fs_count * dspan, quarter)

    widened = tokens.astype(F32)
    mean = lax.psum(jnp.sum(widened * widened, axis=1, keepdims=True), "tp") / (quarter * cols)
    normed = (widened * lax.rsqrt(mean + 1e-06)).astype(BF)
    pad = ((0, 0), (0, wide - toks))
    route = jnp.pad(routes.T.astype(F32), pad, constant_values=-1.0)
    weight = jnp.pad(route_weights.T, pad)
    high = lax.reduce_precision(weight, 8, 7)
    low = weight - high
    meta = jnp.concatenate(
        [
            jnp.concatenate([route, high], axis=1),
            jnp.concatenate([low, jnp.zeros_like(low)], axis=1),
            jnp.zeros((META - 2 * top, quarter), F32),
        ],
        axis=0,
    ).astype(BF)
    sgu = jnp.concatenate([shared_gate * norm_gain[:, None], shared_up * norm_gain[:, None]], axis=1).astype(BF)
    sgu = jnp.concatenate([sgu[: span // 2], sgu[span // 2 :]], axis=1)
    blk = jnp.concatenate([normed, meta, sgu, shared_down.astype(BF)], axis=0)

    dma = pltpu.SemaphoreType.DMA
    slots = chips * 2 * SLOTS
    half = chips // 2
    x, xs, gw, sg, su, sd, gu2 = pl.pallas_call(
        functools.partial(collect_kernel, chips, cols, toks, held, top),
        out_shape=(
            shape(cols, held, slots, quarter), shape(cols, toks, quarter), shape(chips, 2, 4 * SLOTS, wide),
            shape(fs_count * span, lanes), shape(fs_count * span, lanes), shape(fs_count * dspan, quarter),
            shape(*gu.shape),
        ),
        in_specs=[VM] * 2,
        out_specs=(VM,) * 7,
        scratch_shapes=[
            pltpu.VMEM((chips, 2, *blk.shape), BF), pltpu.VMEM((wide, wide), BF),
            dma((2, half)), dma((2, half)), dma((chips,)), dma((chips,)),
            dma((chips + 1,)), dma((chips + 1,)), dma((chips + 1,)), dma((chips + 1,)), dma((chips + 1,)), dma((chips + 1,)),
            dma, dma,
        ],
        compiler_params=pltpu.CompilerParams(collective_id=1, has_side_effects=True, vmem_limit_bytes=48 * 2**20),
        cost_estimate=pl.CostEstimate(flops=60_000_000_000, bytes_accessed=16_000_000, transcendentals=0),
    )(blk, gu)

    parts = 4
    mixed, dn2, od, os = pl.pallas_call(
        functools.partial(layer_kernel, chips, cols),
        out_shape=(
            shape(toks, quarter), shape(*dn.shape), shape(held, lanes, quarter * cols), shape(lanes, quarter * cols),
        ),
        in_specs=[VM] * 9,
        out_specs=(VM,) * 4,
        scratch_shapes=[
            pltpu.VMEM((held, slots, lanes * cols), BF), pltpu.VMEM((toks, lanes * cols), BF),
            pltpu.VMEM((held, slots // parts, quarter), BF), pltpu.VMEM((chips, toks, quarter), F32),
            pltpu.VMEM((chips, toks, quarter), BF), pltpu.VMEM((chips, toks, quarter), BF),
            pltpu.VMEM((half, toks, quarter), BF), pltpu.VMEM((half, toks, quarter), BF),
            pltpu.VMEM((half, toks, quarter), BF), pltpu.VMEM((half, toks, quarter), BF),
            dma((parts + 1,)), dma((parts + 1,)), dma((parts + 1,)), dma((parts + 1,)), dma((parts + 1,)), dma((parts + 1,)),
            dma((chips,)), dma((chips,)), dma((2, half)), dma((2, half)), dma((3, cols - 1)), dma((3, cols - 1)),
            dma, dma,
        ],
        compiler_params=pltpu.CompilerParams(collective_id=2, has_side_effects=True, vmem_limit_bytes=58 * 2**20),
        cost_estimate=pl.CostEstimate(flops=40_000_000_000, bytes_accessed=16_000_000, transcendentals=0),
    )(x, xs, gw, gu, gu2, sg, su, sd, dn)

    first, second = jnp.where(par == 0, gu, gu2), jnp.where(par == 0, gu2, gu)
    gate_ready = jnp.stack([first[:, :lanes], second[:, :lanes]])
    up_ready = jnp.stack([first[:, lanes:], second[:, lanes:]])
    return mixed, gate_ready, up_ready, od, sg, su, os


def solution(mesh):
    return jax.shard_map(
        per_device,
        mesh=mesh,
        in_specs=(
            P(("grp", "fs"), "tp"), P(("grp", "fs"), None), P(("grp", "fs"), None), P("fs"),
            P(None, "fs", "tp"), P(None, "fs", "tp"), P(None, "fs", "tp"),
            P("fs", "tp"), P("fs", "tp"), P("fs", "tp"),
        ),
        out_specs=(
            P(("grp", "fs"), "tp"), P(("grp", "fs"), None, "tp"), P(("grp", "fs"), None, "tp"),
            P(("grp", "fs"), "tp", None), P("grp", "tp"), P("grp", "tp"), P(("grp", "tp"), None),
        ),
        check_vma=False,
    )
```

```python
import functools

import jax
import jax.numpy as jnp
from jax import lax
from jax.experimental import pallas as pl
from jax.experimental.pallas import tpu as pltpu
from jax.sharding import PartitionSpec as P

MESH = pl.DeviceIdType.MESH
BF = jnp.bfloat16
F32 = jnp.float32
META = 16
SLOTS = 32


def remote(src, dst, send_sem, recv_sem, **where):
    return pltpu.make_async_remote_copy(
        src_ref=src, dst_ref=dst, send_sem=send_sem, recv_sem=recv_sem, device_id=where, device_id_type=MESH
    )


def far_first(count):
    half = count // 2
    order = [half]
    for d in range(1, half):
        order += [half - d, half + d]
    return order + [0]


def places(chips, cols):
    g, f, t = lax.axis_index("grp"), lax.axis_index("fs"), lax.axis_index("tp")
    c = lax.rem(f, 2)
    z = lax.div(f, 2)
    up = lax.rem(z + 1, chips) * 2 + c
    down = lax.rem(z + chips - 1, chips) * 2 + c
    other = f + 1 - 2 * c
    par = lax.rem(g, 2)
    pair = g + 1 - 2 * par
    right, left = lax.rem(t + 1, cols), lax.rem(t + cols - 1, cols)
    return f, t, c, z, up, down, other, par, pair, right, left


def greet(peers):
    barrier = pltpu.get_barrier_semaphore()
    for peer in peers:
        pl.semaphore_signal(barrier, inc=1, device_id=peer, device_id_type=MESH)

    def answered():
        pl.semaphore_wait(barrier, len(peers))

    return answered


def whole_kernel(
    chips, cols, held, top,
    tok, routes, weights_of, gain, sgate_own, sup_own, sdown_own, gates, ups, downs,
    mixed, gate_out, up_out, od_out, os_out, sg_out, su_out,
    gf, uf, df, gcast, dcast, table, gu, gu2, od, os, sg, su, in_sem, out_sem, raw, xn, buf, tri, x, gw, sd, dn, dn2, act, sact, y, own, ss, sr, ps, pr, ms, mr,
    gs, gr, ds_, dr, gys, gyr, dys, dyr, ts, tr, zs, zr, cs, cr, rs, rr, ls, lr, fs_, fr,
    ars, arr, als, alr, afs, afr, bs, br, vs, vr, ws, wr,
):
    f, t, c, z, up, down, other, par, pair, right, left = places(chips, cols)
    fs_count = 2 * chips
    half = chips // 2
    order = far_first(chips)
    pos = {r: p for p, r in enumerate(order)}
    toks, quarter = tok.shape
    lanes = sg.shape[1]
    rows = buf.shape[2]
    cut = rows // 2
    width = 2 * SLOTS
    wide = tri.shape[0]
    span, dspan = gcast.shape[1], dcast.shape[1]
    parts = 4
    per = chips // parts
    tall = per * width
    tcut = toks // 2
    across = [lax.rem(t + d, cols) for d in range(1, cols)]

    def core(delta, k):
        return lax.rem(z + delta, chips) * 2 + k

    away = [(delta, k) for delta in range(1, chips) for k in range(2)]
    fetched = [
        pltpu.make_async_copy(src.at[:, par], dst, in_sem.at[n])
        for n, (src, dst) in enumerate(((gates, gf), (ups, uf), (downs, df)))
    ]
    for copy in fetched:
        copy.start()
    answered = greet(
        [{"fs": core(delta, k)} for delta, k in away]
        + [{"fs": other}, {"grp": pair}]
        + [{"tp": a} for a in across]
    )
    sent = []

    def go(copy):
        copy.start()
        sent.append(copy)
        return copy

    def part(ref, owner, size, count=1):
        return ref.at[pl.ds(pl.multiple_of(owner * size, size), count * size), :]

    def hand(cast, target, size, sends, recvs, delta, k):
        there = core(delta, k)
        back = (chips - delta) % chips
        go(remote(cast.at[there], part(target, f, size), sends.at[delta, k], recvs.at[back, c], fs=there))

    def landed(target, size, sends, recvs, delta, k):
        here = part(target, core(delta, k), size)
        remote(here, here, sends.at[delta, k], recvs.at[delta, k], fs=core(delta, k)).wait_recv()

    def hand_gates(d):
        for delta in sorted({d, chips - d}):
            for k in range(2):
                hand(gcast, gu, span, gs, gr, delta, k)

    def swap_chip(target, target2, size, sends, recvs, delta):
        here, there = (part(v, core(delta, 0), size, 2) for v in (target, target2))
        return go(remote(here, there, sends.at[delta], recvs.at[delta], grp=pair))

    table[...] = jnp.full(table.shape, -1.0, F32)
    table[0:toks, 0:top] = routes[...].astype(F32)
    table[0:toks, 8 : 8 + top] = weights_of[...]
    turned = table[...].T
    weight = turned[8:16, :]
    high = weight.astype(BF)
    low = (weight - high.astype(F32)).astype(BF)
    short = span // 2
    scaled = [(v[...] * gain[...]).astype(BF) for v in (sgate_own, sup_own)]
    buf[0, c, toks : toks + 8, 0:wide] = turned[0:8, :].astype(BF)
    buf[0, c, toks : toks + 8, wide:] = high
    buf[0, c, toks + 8 : toks + META, 0:wide] = low
    buf[0, c, toks + 8 : toks + META, wide:] = jnp.zeros_like(low)
    for h in range(2):
        for n in range(2):
            at = (2 * h + n) * lanes
            buf[0, c, toks + META : toks + META + short, at : at + lanes] = scaled[n][h * short : (h + 1) * short]
    buf[0, c, toks + META + short :, :] = sdown_own[...].astype(BF)
    for copy in fetched:
        copy.wait()

    @pl.loop(0, fs_count)
    def _(i):
        gcast[i, :, 0:lanes] = (gf[i] * gain[...]).astype(BF)
        gcast[i, :, lanes:] = (uf[i] * gain[...]).astype(BF)
        dcast[i] = df[i].astype(BF)

    answered()
    traded = [
        go(remote(tok, raw.at[t], ts.at[0], tr.at[0], tp=right)),
        go(remote(tok, raw.at[t], ts.at[1], tr.at[1], tp=left)),
    ]
    for d in range(1, half // 2 + 1):
        hand_gates(d)
    go(remote(gcast.at[other], part(gu, f, span), gs.at[0, 0], gr.at[0, 0], fs=other))
    go(remote(dcast.at[other], part(dn, f, dspan), ds_.at[0, 0], dr.at[0, 0], fs=other))
    part(gu, f, span)[...] = gcast[f]
    part(dn, f, dspan)[...] = dcast[f]
    tri[...] = jnp.where(
        lax.broadcasted_iota(jnp.int32, (wide, wide), 0) < lax.broadcasted_iota(jnp.int32, (wide, wide), 1), 1.0, 0.0
    ).astype(BF)
    traded[0].wait_recv()
    upper, lower = pl.ds(0, tcut), pl.ds(tcut, tcut)
    traded.append(go(remote(raw.at[left, upper], raw.at[left, upper], ts.at[2], tr.at[2], tp=right)))
    traded[1].wait_recv()
    traded.append(go(remote(raw.at[right, lower], raw.at[right, lower], ts.at[3], tr.at[3], tp=left)))
    traded[2].wait_recv()
    traded[3].wait_recv()
    opposite = across[cols // 2 - 1]
    sources = [(t, tok)] + [(q, raw.at[q]) for q in (left, right, opposite)]
    total = jnp.zeros((toks, 1), F32)
    for _, ref in sources:
        value = ref[...].astype(F32)
        total += jnp.sum(value * value, axis=1, keepdims=True)
    scale = lax.rsqrt(total / (quarter * cols) + 1e-06)
    buf[0, c, 0:toks, :] = (tok[...].astype(F32) * scale).astype(BF)
    for q, ref in sources:
        xn[q] = (ref[...].astype(F32) * scale).astype(BF)

    def process(r):
        p = pos[r]

        @pl.loop(0, 2)
        def _(cc):
            meta = buf[r, cc, toks : toks + META, :].astype(F32)
            route, hi, lo = meta[0:8, 0:wide], meta[0:8, wide:], meta[8:META, 0:wide]
            named, his, los = [], [], []
            for j in range(held):
                hit = route == (f * held + j).astype(F32)
                named.append(jnp.sum(jnp.where(hit, 1.0, 0.0), axis=0, keepdims=True))
                his.append(jnp.sum(jnp.where(hit, hi, 0.0), axis=0, keepdims=True))
                los.append(jnp.sum(jnp.where(hit, lo, 0.0), axis=0, keepdims=True))
            stack = jnp.concatenate(named + [jnp.zeros((8 - held, wide), F32)], axis=0)
            rank = jnp.dot(stack.astype(BF), tri[...], preferred_element_type=F32)
            slot = lax.broadcasted_iota(jnp.int32, (SLOTS, wide), 0).astype(F32)
            picks, ghi, glo = [], [], []
            for j in range(held):
                pick = jnp.where(slot == rank[j : j + 1], 1.0, 0.0) * named[j]
                picks.append(pick)
                ghi.append(pick * his[j])
                glo.append(pick * los[j])
            chosen = jnp.concatenate(picks, axis=0).astype(BF)
            gw[p, cc] = jnp.concatenate(ghi + glo, axis=0).astype(BF)
            got = jnp.dot(chosen, buf[r, cc, 0:wide, :], preferred_element_type=F32).astype(BF)
            at = pl.multiple_of(p * width + cc * SLOTS, SLOTS)
            for j in range(held):
                x[t, j, pl.ds(at, SLOTS), :] = got[j * SLOTS : (j + 1) * SLOTS]
            owner = lax.rem(z + r, chips) * 2 + cc
            piece = buf[r, cc, toks + META : toks + META + short, :]
            for h in range(2):
                there = pl.ds(pl.multiple_of(owner * span + h * short, short), short)
                sg[there, :] = piece[:, 2 * h * lanes : (2 * h + 1) * lanes]
                su[there, :] = piece[:, (2 * h + 1) * lanes : (2 * h + 2) * lanes]
            sd[pl.ds(pl.multiple_of(owner * dspan, dspan), dspan), :] = buf[r, cc, toks + META + short :, :]

    def block(q, p):
        return x.at[q, :, pl.ds(p * width, width), :]

    to_right, to_left, onward = {}, {}, {}

    def send_rows(r):
        p = pos[r]
        to_right[p] = go(remote(block(t, p), block(t, p), rs.at[p], rr.at[p], tp=right))
        to_left[p] = go(remote(block(t, p), block(t, p), ls.at[p], lr.at[p], tp=left))

    def pass_rows(p):
        to_right[p].wait_recv()
        to_left[p].wait_recv()
        source, target = (left, right) if p % 2 == 0 else (right, left)
        onward[p] = go(remote(block(source, p), block(source, p), fs_.at[p], fr.at[p], tp=target))

    ring, sib = {}, {}
    bounds = [pl.ds(0, cut), pl.ds(cut, cut)]

    def forward(way, h, d):
        step = chips - d if way == 0 else d
        before = (step + 1) % chips if way == 0 else step - 1
        src, dst = buf.at[before, c, bounds[h]], buf.at[step, c, bounds[h]]
        ring[way, h, d] = go(
            remote(src, dst, zs.at[way, h, d - 1], zr.at[way, h, d - 1], fs=up if way == 0 else down)
        )

    def share(r, h):
        here = buf.at[r, c, bounds[h]]
        sib[r, h] = go(remote(here, here, cs.at[r, h], cr.at[r, h], fs=other))

    flows = [(0, 0), (1, 1), (0, 1), (1, 0)]
    for way, h in flows:
        forward(way, h, 1)
    for h in range(2):
        share(0, h)
    waiting = []
    gate_swaps = {}

    def swap_gates(delta):
        for k in range(2):
            landed(gu, span, gs, gr, delta, k)
        gate_swaps[delta] = swap_chip(gu, gu2, span, gys, gyr, delta)

    remote(part(gu, other, span), part(gu, other, span), gs.at[0, 0], gr.at[0, 0], fs=other).wait_recv()
    gate_swaps[0] = swap_chip(gu, gu2, span, gys, gyr, 0)

    def settle(near):
        for r in near:
            for h in range(2):
                sib[r, h].wait_recv()
            process(r)
        for r in near:
            send_rows(r)
        waiting.extend(pos[r] for r in near)

    def swap_ring(d):
        for delta in sorted({d, chips - d}):
            swap_gates(delta)

    def pass_waiting():
        while waiting:
            pass_rows(waiting.pop(0))

    ready = {half // 2: (1,), half // 2 + 1: (2, 3), half - 2: (4,), half - 1: (5,), half: (6,)} if half == 8 else {}

    def hand_downs():
        for d in range(1, half + 1):
            for delta in sorted({d, chips - d}):
                for k in range(2):
                    hand(dcast, dn, dspan, ds_, dr, delta, k)

    settle([0])
    for d in range(1, half + 1):
        for way, h in flows:
            if d == half and way != h:
                continue
            ring[way, h, d].wait_recv()
            if d + 1 < half or (d + 1 == half and way == h):
                forward(way, h, d + 1)
            share(chips - d if way == 0 else d, h)
        later = half // 2 + (d + 1) // 2
        if d % 2 == 1 and later <= half:
            hand_gates(later)
        if d == half - 1:
            hand_downs()
        pass_waiting()
        settle([chips - d, d] if d < half else [half])
        for n in ready.get(d, ()):
            swap_ring(n)
    onward[pos[half]] = go(
        remote(block(t, pos[half]), block(t, pos[half]), fs_.at[pos[half]], fr.at[pos[half]], tp=opposite)
    )
    for n in range(1, half + 1):
        if n not in sum(ready.values(), ()):
            swap_ring(n)
    to_right[pos[half]].wait_recv()
    to_left[pos[half]].wait_recv()
    for p in onward:
        onward[p].wait_recv()
    down_swaps = []

    def land_downs(d):
        for delta in sorted({d, chips - d} if d else {0}):
            if delta:
                for k in range(2):
                    landed(dn, dspan, ds_, dr, delta, k)
            else:
                remote(part(dn, other, dspan), part(dn, other, dspan), ds_.at[0, 0], dr.at[0, 0], fs=other).wait_recv()
            down_swaps.append(swap_chip(dn, dn2, dspan, dys, dyr, delta))

    for d in range(half // 2):
        land_downs(d)

    own_lanes = pl.ds(pl.multiple_of(t * lanes, lanes), lanes)

    def hidden(j, at, weights):
        both = jnp.zeros((tall, 2 * lanes), F32)
        for q in range(cols):
            both += jnp.dot(x[q, j, at, :], weights[q * quarter : (q + 1) * quarter, :], preferred_element_type=F32)
        act[j, at, own_lanes] = (jax.nn.silu(both[:, :lanes]) * both[:, lanes:]).astype(BF)

    @pl.loop(0, parts)
    def _(i):
        hidden(par, pl.ds(pl.multiple_of(i * tall, tall), tall), gu)

    for delta in gate_swaps:
        gate_swaps[delta].wait_recv()
    outs = []

    def leave(src, dst):
        copy = pltpu.make_async_copy(src, dst, out_sem.at[len(outs)])
        copy.start()
        outs.append(copy)

    to_right2, to_left2, onward2 = {}, {}, {}

    def piece(q, i):
        cols_of = pl.ds(pl.multiple_of(q * lanes, lanes), lanes)
        return sact.at[:, cols_of] if i == parts else act.at[:, pl.ds(i * tall, tall), cols_of]

    def send_act(i):
        to_right2[i] = go(remote(piece(t, i), piece(t, i), ars.at[i], arr.at[i], tp=right))
        to_left2[i] = go(remote(piece(t, i), piece(t, i), als.at[i], alr.at[i], tp=left))

    def pass_act(i):
        to_right2[i].wait_recv()
        to_left2[i].wait_recv()
        if i == 0:
            return
        source, target = (left, right) if i % 2 == 0 else (right, left)
        onward2[i] = go(remote(piece(source, i), piece(source, i), afs.at[i], afr.at[i], tp=target))

    for i in range(parts):
        hidden(1 - par, pl.ds(i * tall, tall), gu2)
        send_act(i)
        if i == 0:
            onward2[0] = go(remote(piece(t, 0), piece(t, 0), afs.at[0], afr.at[0], tp=opposite))
    sgate = jnp.zeros((toks, lanes), F32)
    sup = jnp.zeros((toks, lanes), F32)
    for q in range(cols):
        there = slice(q * quarter, (q + 1) * quarter)
        sgate += jnp.dot(xn[q], sg[there, :], preferred_element_type=F32)
        sup += jnp.dot(xn[q], su[there, :], preferred_element_type=F32)
    sact[:, own_lanes] = (jax.nn.silu(sgate) * sup).astype(BF)
    send_act(parts)
    placed = []

    def place(kind, source, target):
        home = pl.ds(pl.multiple_of(t * quarter, quarter), quarter)
        for k, a in enumerate(across):
            rows_of = pl.ds(pl.multiple_of(a * lanes, lanes), lanes)
            placed.append(go(remote(source.at[rows_of, :], target.at[:, home], ws.at[kind, k], wr.at[kind, k], tp=a)))
        target[:, home] = source[pl.ds(pl.multiple_of(t * lanes, lanes), lanes), :]

    land_downs(half // 2)
    land_downs(half // 2 + 1)
    pass_act(0)
    land_downs(half // 2 + 2)
    pass_act(1)
    for d in range(half // 2 + 3, half + 1):
        land_downs(d)
    for copy in down_swaps:
        copy.wait_recv()
    sibs = {}

    def chunk(i):
        onward2[i].wait_recv()
        for j, weights in ((par, dn), (1 - par, dn2)):
            y[j] = jnp.dot(act[j, i * tall : (i + 1) * tall, :], weights[...], preferred_element_type=F32).astype(BF)

        def combine(p, u, cc):
            at = pl.ds(pl.multiple_of(u * width + cc * SLOTS, SLOTS), SLOTS)
            found = jnp.concatenate([y[0, at, :], y[1, at, :]], axis=0)
            twice = jnp.concatenate([found, found], axis=0)
            whole = lax.dot_general(gw[p, cc], twice, (((0,), (0,)), ((), ())), preferred_element_type=F32)
            return whole[0:toks]

        for u in range(per):
            p = i * per + u
            ss[p] = combine(p, u, 1 - c).astype(BF)
            sibs[p] = go(remote(ss.at[p], sr.at[p], bs.at[p], br.at[p], fs=other))
            own[p] = combine(p, u, c)
            if p == 1:
                step(0)

    sums = {}
    limits = [slice(0, tcut), slice(tcut, toks)]
    met = set()

    def local(r, h):
        p = pos[r]
        if p not in met:
            met.add(p)
            sibs[p].wait_recv()
        return own[p, limits[h], :] + sr[p, limits[h], :].astype(F32)

    def add_on(way, h, r):
        out, into = ((ps, pr), (ms, mr))[way]
        k = half - r if way == 0 else r - half
        value = local(r, h)
        first = way != h and k == 1 or k == 0
        if not first:
            sums[way, h, k - 1].wait_recv()
            value = value + into[k - 1, limits[h], :].astype(F32)
        out[k, limits[h], :] = value.astype(BF)
        there = (upper, lower)[h]
        sums[way, h, k] = go(
            remote(out.at[k, there], into.at[k, there], vs.at[way, h, k], vr.at[way, h, k], fs=up if way == 0 else down)
        )

    def step(k):
        for way, h in flows:
            if k == 0 and way != h:
                continue
            add_on(way, h, half - k if way == 0 else half + k)

    done = 1
    for i in range(parts):
        if i + 2 <= parts:
            pass_act(i + 2)
        chunk(i)
        while done < half and max(pos[half - done], pos[(half + done) % chips]) < (i + 1) * per and done <= 2 * i:
            step(done)
            done += 1
        if i == 0:
            place(0, dn, od.at[par])
            place(1, dn2, od.at[1 - par])
            place(2, sd, os)
            for n, (mine, theirs, target) in enumerate(
                ((gu, gu2, gate_out), (gu, gu2, up_out))
            ):
                these = pl.ds(n * lanes, lanes)
                leave(mine.at[:, these], target.at[par])
                leave(theirs.at[:, these], target.at[1 - par])
            leave(sg, sg_out)
            leave(su, su_out)
    onward2[parts].wait_recv()
    shared = jnp.dot(sact[...], sd[...], preferred_element_type=F32)
    own[pos[0]] = own[pos[0]] + shared
    while done < half:
        step(done)
        done += 1
    for copy in placed:
        copy.wait_recv()
    leave(od, od_out)
    leave(os, os_out)
    for h in range(2):
        value = local(0, h)
        for way in range(2):
            sums[way, h, half - 1].wait_recv()
            value = value + (pr, mr)[way][half - 1, limits[h], :].astype(F32)
        mixed[limits[h], :] = value.astype(BF)
    for copy in outs:
        copy.wait()
    for copy in sent:
        copy.wait_send()


VM = pl.BlockSpec(memory_space=pltpu.VMEM)
ANY = pl.BlockSpec(memory_space=pl.ANY)


def shape(*dims, kind=BF):
    return jax.ShapeDtypeStruct(dims, kind)


def per_device(
    tokens, routes, route_weights, norm_gain, gate_experts, up_experts, down_experts, shared_gate, shared_up, shared_down
):
    fs_count, cols = lax.axis_size("fs"), lax.axis_size("tp")
    chips = fs_count // 2
    experts, span, lanes = gate_experts.shape
    held = experts // fs_count
    toks, quarter = tokens.shape
    top = routes.shape[1]
    dspan = down_experts.shape[1]
    wide = quarter // 2

    def pairs_of(w):
        return w.reshape(fs_count, held, *w.shape[1:])

    def dma(*dims):
        return pltpu.SemaphoreType.DMA(dims)

    slots = chips * 2 * SLOTS
    half = chips // 2
    parts = 4
    rows = toks + META + span // 2 + dspan
    full, dfull = fs_count * span, fs_count * dspan
    ring = [pltpu.VMEM((half, toks, quarter), BF)] * 4
    mixed, gate_ready, up_ready, od, os, sg, su = pl.pallas_call(
        functools.partial(whole_kernel, chips, cols, held, top),
        out_shape=(
            shape(toks, quarter), shape(held, full, lanes), shape(held, full, lanes), shape(held, lanes, quarter * cols),
            shape(lanes, quarter * cols), shape(full, lanes), shape(full, lanes),
        ),
        in_specs=[VM] * 7 + [ANY] * 3,
        out_specs=(VM,) + (ANY,) * 6,
        scratch_shapes=[
            pltpu.VMEM((fs_count, span, lanes), F32), pltpu.VMEM((fs_count, span, lanes), F32),
            pltpu.VMEM((fs_count, dspan, quarter), F32),
            pltpu.VMEM((fs_count, span, 2 * lanes), BF), pltpu.VMEM((fs_count, dspan, quarter), BF),
            pltpu.VMEM((wide, 128), F32), pltpu.VMEM((full, 2 * lanes), BF), pltpu.VMEM((full, 2 * lanes), BF),
            pltpu.VMEM((held, lanes, quarter * cols), BF), pltpu.VMEM((lanes, quarter * cols), BF),
            pltpu.VMEM((full, lanes), BF), pltpu.VMEM((full, lanes), BF), dma(3), dma(8),
            pltpu.VMEM((cols, toks, quarter), BF), pltpu.VMEM((cols, toks, quarter), BF),
            pltpu.VMEM((chips, 2, rows, quarter), BF), pltpu.VMEM((wide, wide), BF),
            pltpu.VMEM((cols, held, slots, quarter), BF), pltpu.VMEM((chips, 2, 4 * SLOTS, wide), BF),
            pltpu.VMEM((dfull, quarter), BF), pltpu.VMEM((dfull, quarter), BF), pltpu.VMEM((dfull, quarter), BF),
            pltpu.VMEM((held, slots, lanes * cols), BF), pltpu.VMEM((toks, lanes * cols), BF),
            pltpu.VMEM((held, slots // parts, quarter), BF), pltpu.VMEM((chips, toks, quarter), F32),
            pltpu.VMEM((chips, toks, quarter), BF), pltpu.VMEM((chips, toks, quarter), BF), *ring,
            dma(chips, 2), dma(chips, 2), dma(chips, 2), dma(chips, 2), dma(chips), dma(chips), dma(chips), dma(chips),
            dma(4), dma(4), dma(2, 2, half), dma(2, 2, half), dma(chips, 2), dma(chips, 2),
            *[dma(chips)] * 6, *[dma(parts + 1)] * 6, dma(chips), dma(chips), dma(2, 2, half), dma(2, 2, half),
            dma(3, cols - 1), dma(3, cols - 1),
        ],
        compiler_params=pltpu.CompilerParams(collective_id=1, has_side_effects=True, vmem_limit_bytes=62 * 2**20),
        cost_estimate=pl.CostEstimate(flops=60_000_000_000, bytes_accessed=16_000_000, transcendentals=0),
    )(
        tokens, routes, route_weights, norm_gain.reshape(span, 1), shared_gate, shared_up, shared_down,
        pairs_of(gate_experts), pairs_of(up_experts), pairs_of(down_experts),
    )
    return mixed, gate_ready, up_ready, od, sg, su, os


def solution(mesh):
    return jax.shard_map(
        per_device,
        mesh=mesh,
        in_specs=(
            P(("grp", "fs"), "tp"), P(("grp", "fs"), None), P(("grp", "fs"), None), P("fs"),
            P(None, "fs", "tp"), P(None, "fs", "tp"), P(None, "fs", "tp"),
            P("fs", "tp"), P("fs", "tp"), P("fs", "tp"),
        ),
        out_specs=(
            P(("grp", "fs"), "tp"), P(("grp", "fs"), None, "tp"), P(("grp", "fs"), None, "tp"),
            P(("grp", "fs"), "tp", None), P("grp", "tp"), P("grp", "tp"), P(("grp", "tp"), None),
        ),
        check_vma=False,
    )
```

```python
import functools

import jax
import jax.numpy as jnp
from jax import lax
from jax.experimental import pallas as pl
from jax.experimental.pallas import tpu as pltpu
from jax.sharding import PartitionSpec as P

MESH = pl.DeviceIdType.MESH
BF = jnp.bfloat16
F32 = jnp.float32
META = 16
SLOTS = 32


def remote(src, dst, send_sem, recv_sem, **where):
    return pltpu.make_async_remote_copy(
        src_ref=src, dst_ref=dst, send_sem=send_sem, recv_sem=recv_sem, device_id=where, device_id_type=MESH
    )


def far_first(count):
    half = count // 2
    order = [half]
    for d in range(1, half):
        order += [half - d, half + d]
    return order + [0]


def places(chips, cols):
    g, f, t = lax.axis_index("grp"), lax.axis_index("fs"), lax.axis_index("tp")
    c = lax.rem(f, 2)
    z = lax.div(f, 2)
    up = lax.rem(z + 1, chips) * 2 + c
    down = lax.rem(z + chips - 1, chips) * 2 + c
    other = f + 1 - 2 * c
    par = lax.rem(g, 2)
    pair = g + 1 - 2 * par
    right, left = lax.rem(t + 1, cols), lax.rem(t + cols - 1, cols)
    return f, t, c, z, up, down, other, par, pair, right, left


def greet(peers):
    barrier = pltpu.get_barrier_semaphore()
    for peer in peers:
        pl.semaphore_signal(barrier, inc=1, device_id=peer, device_id_type=MESH)

    def answered():
        pl.semaphore_wait(barrier, len(peers))

    return answered


def whole_kernel(
    chips, cols, held, top,
    tok, routes, weights_of, gain, sgate_own, sup_own, sdown_own, gates, ups, downs,
    mixed, gate_out, up_out, od_out, os_out, sg_out, su_out,
    gf, uf, df, gcast, dcast, table, gu, gu2, od, os, sg, su, in_sem, out_sem, raw, xn, buf, tri, x, gw, sd, dn, dn2, act, sact, y, own, ss, sr, ps, pr, ms, mr,
    gs, gr, ds_, dr, gys, gyr, dys, dyr, ts, tr, zs, zr, cs, cr, rs, rr, ls, lr, fs_, fr,
    ars, arr, als, alr, afs, afr, bs, br, vs, vr, ws, wr,
):
    f, t, c, z, up, down, other, par, pair, right, left = places(chips, cols)
    fs_count = 2 * chips
    half = chips // 2
    order = far_first(chips)
    pos = {r: p for p, r in enumerate(order)}
    toks, quarter = tok.shape
    lanes = sg.shape[1]
    rows = buf.shape[2]
    cut = rows // 2
    width = 2 * SLOTS
    wide = tri.shape[0]
    span, dspan = gcast.shape[1], dcast.shape[1]
    parts = 4
    per = chips // parts
    tall = per * width
    tcut = toks // 2
    across = [lax.rem(t + d, cols) for d in range(1, cols)]

    def core(delta, k):
        return lax.rem(z + delta, chips) * 2 + k

    away = [(delta, k) for delta in range(1, chips) for k in range(2)]
    fetched = [
        pltpu.make_async_copy(src.at[:, par], dst, in_sem.at[n])
        for n, (src, dst) in enumerate(((gates, gf), (ups, uf), (downs, df)))
    ]
    for copy in fetched:
        copy.start()
    answered = greet(
        [{"fs": core(delta, k)} for delta, k in away]
        + [{"fs": other}, {"grp": pair}]
        + [{"tp": a} for a in across]
    )
    sent = []

    def go(copy):
        copy.start()
        sent.append(copy)
        return copy

    def part(ref, owner, size, count=1):
        return ref.at[pl.ds(pl.multiple_of(owner * size, size), count * size), :]

    def hand(cast, target, size, sends, recvs, delta, k):
        there = core(delta, k)
        back = (chips - delta) % chips
        go(remote(cast.at[there], part(target, f, size), sends.at[delta, k], recvs.at[back, c], fs=there))

    def landed(target, size, sends, recvs, delta, k):
        here = part(target, core(delta, k), size)
        remote(here, here, sends.at[delta, k], recvs.at[delta, k], fs=core(delta, k)).wait_recv()

    def hand_gates(d):
        for delta in sorted({d, chips - d}):
            for k in range(2):
                hand(gcast, gu, span, gs, gr, delta, k)

    def swap_chip(target, target2, size, sends, recvs, delta):
        here, there = (part(v, core(delta, 0), size, 2) for v in (target, target2))
        return go(remote(here, there, sends.at[delta], recvs.at[delta], grp=pair))

    table[...] = jnp.full(table.shape, -1.0, F32)
    table[0:top, 0:toks] = routes[...].astype(F32)
    table[8 : 8 + top, 0:toks] = weights_of[...]
    turned = table[...]
    diagonal = lax.broadcasted_iota(jnp.int32, (span, span), 0) == lax.broadcasted_iota(jnp.int32, (span, span), 1)
    column = jnp.sum(jnp.where(diagonal, jnp.broadcast_to(gain[...], (span, span)), 0.0), axis=1, keepdims=True)
    weight = turned[8:16, :]
    high = weight.astype(BF)
    low = (weight - high.astype(F32)).astype(BF)
    short = span // 2
    scaled = [(v[...] * column).astype(BF) for v in (sgate_own, sup_own)]
    buf[0, c, toks : toks + 8, 0:wide] = turned[0:8, :].astype(BF)
    buf[0, c, toks : toks + 8, wide:] = high
    buf[0, c, toks + 8 : toks + META, 0:wide] = low
    buf[0, c, toks + 8 : toks + META, wide:] = jnp.zeros_like(low)
    for h in range(2):
        for n in range(2):
            at = (2 * h + n) * lanes
            buf[0, c, toks + META : toks + META + short, at : at + lanes] = scaled[n][h * short : (h + 1) * short]
    buf[0, c, toks + META + short :, :] = sdown_own[...].astype(BF)
    for copy in fetched:
        copy.wait()

    @pl.loop(0, fs_count)
    def _(i):
        gcast[i, :, 0:lanes] = (gf[i] * column).astype(BF)
        gcast[i, :, lanes:] = (uf[i] * column).astype(BF)
        dcast[i] = df[i].astype(BF)

    answered()
    traded = [
        go(remote(tok, raw.at[t], ts.at[0], tr.at[0], tp=right)),
        go(remote(tok, raw.at[t], ts.at[1], tr.at[1], tp=left)),
    ]
    for d in range(1, half // 2 + 1):
        hand_gates(d)
    go(remote(gcast.at[other], part(gu, f, span), gs.at[0, 0], gr.at[0, 0], fs=other))
    go(remote(dcast.at[other], part(dn, f, dspan), ds_.at[0, 0], dr.at[0, 0], fs=other))
    part(gu, f, span)[...] = gcast[f]
    part(dn, f, dspan)[...] = dcast[f]
    tri[...] = jnp.where(
        lax.broadcasted_iota(jnp.int32, (wide, wide), 0) < lax.broadcasted_iota(jnp.int32, (wide, wide), 1), 1.0, 0.0
    ).astype(BF)
    traded[0].wait_recv()
    upper, lower = pl.ds(0, tcut), pl.ds(tcut, tcut)
    traded.append(go(remote(raw.at[left, upper], raw.at[left, upper], ts.at[2], tr.at[2], tp=right)))
    traded[1].wait_recv()
    traded.append(go(remote(raw.at[right, lower], raw.at[right, lower], ts.at[3], tr.at[3], tp=left)))
    traded[2].wait_recv()
    traded[3].wait_recv()
    opposite = across[cols // 2 - 1]
    sources = [(t, tok)] + [(q, raw.at[q]) for q in (left, right, opposite)]
    total = jnp.zeros((toks, 1), F32)
    for _, ref in sources:
        value = ref[...].astype(F32)
        total += jnp.sum(value * value, axis=1, keepdims=True)
    scale = lax.rsqrt(total / (quarter * cols) + 1e-06)
    buf[0, c, 0:toks, :] = (tok[...].astype(F32) * scale).astype(BF)
    for q, ref in sources:
        xn[q] = (ref[...].astype(F32) * scale).astype(BF)

    def process(r):
        p = pos[r]

        @pl.loop(0, 2)
        def _(cc):
            meta = buf[r, cc, toks : toks + META, :].astype(F32)
            route, hi, lo = meta[0:8, 0:wide], meta[0:8, wide:], meta[8:META, 0:wide]
            named, his, los = [], [], []
            for j in range(held):
                hit = route == (f * held + j).astype(F32)
                named.append(jnp.sum(jnp.where(hit, 1.0, 0.0), axis=0, keepdims=True))
                his.append(jnp.sum(jnp.where(hit, hi, 0.0), axis=0, keepdims=True))
                los.append(jnp.sum(jnp.where(hit, lo, 0.0), axis=0, keepdims=True))
            stack = jnp.concatenate(named + [jnp.zeros((8 - held, wide), F32)], axis=0)
            rank = jnp.dot(stack.astype(BF), tri[...], preferred_element_type=F32)
            slot = lax.broadcasted_iota(jnp.int32, (SLOTS, wide), 0).astype(F32)
            picks, ghi, glo = [], [], []
            for j in range(held):
                pick = jnp.where(slot == rank[j : j + 1], 1.0, 0.0) * named[j]
                picks.append(pick)
                ghi.append(pick * his[j])
                glo.append(pick * los[j])
            chosen = jnp.concatenate(picks, axis=0).astype(BF)
            gw[p, cc] = jnp.concatenate(ghi + glo, axis=0).astype(BF)
            got = jnp.dot(chosen, buf[r, cc, 0:wide, :], preferred_element_type=F32).astype(BF)
            at = pl.multiple_of(p * width + cc * SLOTS, SLOTS)
            for j in range(held):
                x[t, j, pl.ds(at, SLOTS), :] = got[j * SLOTS : (j + 1) * SLOTS]
            owner = lax.rem(z + r, chips) * 2 + cc
            piece = buf[r, cc, toks + META : toks + META + short, :]
            for h in range(2):
                there = pl.ds(pl.multiple_of(owner * span + h * short, short), short)
                sg[there, :] = piece[:, 2 * h * lanes : (2 * h + 1) * lanes]
                su[there, :] = piece[:, (2 * h + 1) * lanes : (2 * h + 2) * lanes]
            sd[pl.ds(pl.multiple_of(owner * dspan, dspan), dspan), :] = buf[r, cc, toks + META + short :, :]

    def block(q, p):
        return x.at[q, :, pl.ds(p * width, width), :]

    to_right, to_left, onward = {}, {}, {}

    def send_rows(r):
        p = pos[r]
        to_right[p] = go(remote(block(t, p), block(t, p), rs.at[p], rr.at[p], tp=right))
        to_left[p] = go(remote(block(t, p), block(t, p), ls.at[p], lr.at[p], tp=left))

    def pass_rows(p):
        to_right[p].wait_recv()
        to_left[p].wait_recv()
        source, target = (left, right) if p % 2 == 0 else (right, left)
        onward[p] = go(remote(block(source, p), block(source, p), fs_.at[p], fr.at[p], tp=target))

    ring, sib = {}, {}
    bounds = [pl.ds(0, cut), pl.ds(cut, cut)]

    def forward(way, h, d):
        step = chips - d if way == 0 else d
        before = (step + 1) % chips if way == 0 else step - 1
        src, dst = buf.at[before, c, bounds[h]], buf.at[step, c, bounds[h]]
        ring[way, h, d] = go(
            remote(src, dst, zs.at[way, h, d - 1], zr.at[way, h, d - 1], fs=up if way == 0 else down)
        )

    def share(r, h):
        here = buf.at[r, c, bounds[h]]
        sib[r, h] = go(remote(here, here, cs.at[r, h], cr.at[r, h], fs=other))

    flows = [(0, 0), (1, 1), (0, 1), (1, 0)]
    for way, h in flows:
        forward(way, h, 1)
    for h in range(2):
        share(0, h)
    waiting = []
    gate_swaps = {}

    def swap_gates(delta):
        for k in range(2):
            landed(gu, span, gs, gr, delta, k)
        gate_swaps[delta] = swap_chip(gu, gu2, span, gys, gyr, delta)

    remote(part(gu, other, span), part(gu, other, span), gs.at[0, 0], gr.at[0, 0], fs=other).wait_recv()
    gate_swaps[0] = swap_chip(gu, gu2, span, gys, gyr, 0)

    def settle(near):
        for r in near:
            for h in range(2):
                sib[r, h].wait_recv()
            process(r)
        for r in near:
            send_rows(r)
        waiting.extend(pos[r] for r in near)

    def swap_ring(d):
        for delta in sorted({d, chips - d}):
            swap_gates(delta)

    def pass_waiting():
        while waiting:
            pass_rows(waiting.pop(0))

    ready = {half // 2: (1,), half // 2 + 1: (2, 3), half - 2: (4,), half - 1: (5,), half: (6,)} if half == 8 else {}

    def hand_downs():
        for d in range(1, half + 1):
            for delta in sorted({d, chips - d}):
                for k in range(2):
                    hand(dcast, dn, dspan, ds_, dr, delta, k)

    settle([0])
    for d in range(1, half + 1):
        for way, h in flows:
            if d == half and way != h:
                continue
            ring[way, h, d].wait_recv()
            if d + 1 < half or (d + 1 == half and way == h):
                forward(way, h, d + 1)
            share(chips - d if way == 0 else d, h)
        later = half // 2 + (d + 1) // 2
        if d % 2 == 1 and later <= half:
            hand_gates(later)
        if d == half - 1:
            hand_downs()
        if d < half:
            pass_waiting()
            settle([chips - d, d])
        else:
            settle([half])
        for n in ready.get(d, ()):
            swap_ring(n)
    onward[pos[half]] = go(
        remote(block(t, pos[half]), block(t, pos[half]), fs_.at[pos[half]], fr.at[pos[half]], tp=opposite)
    )
    waiting.remove(pos[half])
    pass_waiting()
    for n in range(1, half + 1):
        if n not in sum(ready.values(), ()):
            swap_ring(n)
    down_swaps = []

    def land_downs(d):
        for delta in sorted({d, chips - d} if d else {0}):
            if delta:
                for k in range(2):
                    landed(dn, dspan, ds_, dr, delta, k)
            else:
                remote(part(dn, other, dspan), part(dn, other, dspan), ds_.at[0, 0], dr.at[0, 0], fs=other).wait_recv()
            down_swaps.append(swap_chip(dn, dn2, dspan, dys, dyr, delta))

    for d in range(3):
        land_downs(d)
    to_right[pos[half]].wait_recv()
    to_left[pos[half]].wait_recv()
    for p in onward:
        onward[p].wait_recv()
    for d in range(3, half // 2 + 1):
        land_downs(d)

    own_lanes = pl.ds(pl.multiple_of(t * lanes, lanes), lanes)

    def hidden(j, at, weights):
        both = jnp.zeros((tall, 2 * lanes), F32)
        for q in range(cols):
            both += jnp.dot(x[q, j, at, :], weights[q * quarter : (q + 1) * quarter, :], preferred_element_type=F32)
        act[j, at, own_lanes] = (jax.nn.silu(both[:, :lanes]) * both[:, lanes:]).astype(BF)

    @pl.loop(0, parts)
    def _(i):
        hidden(par, pl.ds(pl.multiple_of(i * tall, tall), tall), gu)

    for delta in gate_swaps:
        gate_swaps[delta].wait_recv()
    land_downs(half // 2 + 1)
    outs = []

    def leave(src, dst):
        copy = pltpu.make_async_copy(src, dst, out_sem.at[len(outs)])
        copy.start()
        outs.append(copy)

    to_right2, to_left2, onward2 = {}, {}, {}

    def piece(q, i):
        cols_of = pl.ds(pl.multiple_of(q * lanes, lanes), lanes)
        return sact.at[:, cols_of] if i == parts else act.at[:, pl.ds(i * tall, tall), cols_of]

    def send_act(i):
        to_right2[i] = go(remote(piece(t, i), piece(t, i), ars.at[i], arr.at[i], tp=right))
        to_left2[i] = go(remote(piece(t, i), piece(t, i), als.at[i], alr.at[i], tp=left))

    def pass_act(i):
        to_right2[i].wait_recv()
        to_left2[i].wait_recv()
        if i == 0:
            return
        source, target = (left, right) if i % 2 == 0 else (right, left)
        onward2[i] = go(remote(piece(source, i), piece(source, i), afs.at[i], afr.at[i], tp=target))

    for i in range(parts):
        hidden(1 - par, pl.ds(i * tall, tall), gu2)
        send_act(i)
        if i == 0:
            onward2[0] = go(remote(piece(t, 0), piece(t, 0), afs.at[0], afr.at[0], tp=opposite))
    sgate = jnp.zeros((toks, lanes), F32)
    sup = jnp.zeros((toks, lanes), F32)
    for q in range(cols):
        there = slice(q * quarter, (q + 1) * quarter)
        sgate += jnp.dot(xn[q], sg[there, :], preferred_element_type=F32)
        sup += jnp.dot(xn[q], su[there, :], preferred_element_type=F32)
    sact[:, own_lanes] = (jax.nn.silu(sgate) * sup).astype(BF)
    send_act(parts)
    placed = []

    def place(kind, source, target):
        home = pl.ds(pl.multiple_of(t * quarter, quarter), quarter)
        for k, a in enumerate(across):
            rows_of = pl.ds(pl.multiple_of(a * lanes, lanes), lanes)
            placed.append(go(remote(source.at[rows_of, :], target.at[:, home], ws.at[kind, k], wr.at[kind, k], tp=a)))
        target[:, home] = source[pl.ds(pl.multiple_of(t * lanes, lanes), lanes), :]

    for d in range(half // 2 + 2, half + 1):
        land_downs(d)
    pass_act(0)
    for copy in down_swaps:
        copy.wait_recv()
    sibs = {}

    def chunk(i):
        onward2[i].wait_recv()
        for j, weights in ((par, dn), (1 - par, dn2)):
            y[j] = jnp.dot(act[j, i * tall : (i + 1) * tall, :], weights[...], preferred_element_type=F32).astype(BF)

        def combine(p, u, cc):
            at = pl.ds(pl.multiple_of(u * width + cc * SLOTS, SLOTS), SLOTS)
            found = jnp.concatenate([y[0, at, :], y[1, at, :]], axis=0)
            twice = jnp.concatenate([found, found], axis=0)
            whole = lax.dot_general(gw[p, cc], twice, (((0,), (0,)), ((), ())), preferred_element_type=F32)
            return whole[0:toks]

        for u in range(per):
            p = i * per + u
            ss[p] = combine(p, u, 1 - c).astype(BF)
            sibs[p] = go(remote(ss.at[p], sr.at[p], bs.at[p], br.at[p], fs=other))
            own[p] = combine(p, u, c)
            if p == 1:
                step(0)

    sums = {}
    limits = [slice(0, tcut), slice(tcut, toks)]
    met = set()

    def local(r, h):
        p = pos[r]
        if p not in met:
            met.add(p)
            sibs[p].wait_recv()
        return own[p, limits[h], :] + sr[p, limits[h], :].astype(F32)

    def add_on(way, h, r):
        out, into = ((ps, pr), (ms, mr))[way]
        k = half - r if way == 0 else r - half
        value = local(r, h)
        first = way != h and k == 1 or k == 0
        if not first:
            sums[way, h, k - 1].wait_recv()
            value = value + into[k - 1, limits[h], :].astype(F32)
        out[k, limits[h], :] = value.astype(BF)
        there = (upper, lower)[h]
        sums[way, h, k] = go(
            remote(out.at[k, there], into.at[k, there], vs.at[way, h, k], vr.at[way, h, k], fs=up if way == 0 else down)
        )

    def step(k):
        for way, h in flows:
            if k == 0 and way != h:
                continue
            add_on(way, h, half - k if way == 0 else half + k)

    done = 1
    for i in range(parts):
        chunk(i)
        if i == 0:
            pass_act(1)
            pass_act(2)
        while done < half and max(pos[half - done], pos[(half + done) % chips]) < (i + 1) * per and done <= 2 * i:
            step(done)
            done += 1
        if i == 0:
            place(0, dn, od.at[par])
            place(1, dn2, od.at[1 - par])
            place(2, sd, os)
            for n, (mine, theirs, target) in enumerate(
                ((gu, gu2, gate_out), (gu, gu2, up_out))
            ):
                these = pl.ds(n * lanes, lanes)
                leave(mine.at[:, these], target.at[par])
                leave(theirs.at[:, these], target.at[1 - par])
            pass_act(3)
            pass_act(4)
            leave(sg, sg_out)
            leave(su, su_out)
    onward2[parts].wait_recv()
    shared = jnp.dot(sact[...], sd[...], preferred_element_type=F32)
    own[pos[0]] = own[pos[0]] + shared
    while done < half:
        step(done)
        done += 1
    for copy in placed:
        copy.wait_recv()
    leave(od, od_out)
    leave(os, os_out)
    for h in range(2):
        value = local(0, h)
        for way in range(2):
            sums[way, h, half - 1].wait_recv()
            value = value + (pr, mr)[way][half - 1, limits[h], :].astype(F32)
        mixed[limits[h], :] = value.astype(BF)
    for copy in outs:
        copy.wait()
    for copy in sent:
        copy.wait_send()


VM = pl.BlockSpec(memory_space=pltpu.VMEM)
ANY = pl.BlockSpec(memory_space=pl.ANY)


def shape(*dims, kind=BF):
    return jax.ShapeDtypeStruct(dims, kind)


def finish_kernel(count, *refs):
    ins, outs, bufs = refs[:count], refs[count : 2 * count], refs[2 * count : 3 * count]
    in_sem, out_sem = refs[3 * count :]
    reads = [pltpu.make_async_copy(ins[n], bufs[n], in_sem.at[n]) for n in range(count)]
    writes = [pltpu.make_async_copy(bufs[n], outs[n], out_sem.at[n]) for n in range(count)]
    for copy in reads:
        copy.start()
    for n in range(count):
        reads[n].wait()
        writes[n].start()
    for copy in writes:
        copy.wait()


def finish(*arrays):
    count = len(arrays)
    sems = [pltpu.SemaphoreType.DMA((count,))] * 2
    return pl.pallas_call(
        functools.partial(finish_kernel, count),
        out_shape=tuple(shape(*a.shape, kind=a.dtype) for a in arrays),
        in_specs=[ANY] * count,
        out_specs=(ANY,) * count,
        scratch_shapes=[pltpu.VMEM(a.shape, a.dtype) for a in arrays] + sems,
    )(*arrays)


def per_device(
    tokens, routes, route_weights, norm_gain, gate_experts, up_experts, down_experts, shared_gate, shared_up, shared_down
):
    fs_count, cols = lax.axis_size("fs"), lax.axis_size("tp")
    chips = fs_count // 2
    experts, span, lanes = gate_experts.shape
    held = experts // fs_count
    toks, quarter = tokens.shape
    top = routes.shape[1]
    dspan = down_experts.shape[1]
    wide = quarter // 2

    def pairs_of(w):
        return w.reshape(fs_count, held, *w.shape[1:])

    def dma(*dims):
        return pltpu.SemaphoreType.DMA(dims)

    slots = chips * 2 * SLOTS
    half = chips // 2
    parts = 4
    rows = toks + META + span // 2 + dspan
    full, dfull = fs_count * span, fs_count * dspan
    ring = [pltpu.VMEM((half, toks, quarter), BF)] * 4
    mixed, gate_ready, up_ready, od, os, sg, su = pl.pallas_call(
        functools.partial(whole_kernel, chips, cols, held, top),
        out_shape=(
            shape(toks, quarter), shape(held, full, lanes), shape(held, full, lanes), shape(held, lanes, quarter * cols),
            shape(lanes, quarter * cols), shape(full, lanes), shape(full, lanes),
        ),
        in_specs=[VM] * 7 + [ANY] * 3,
        out_specs=(VM,) + (ANY,) * 6,
        scratch_shapes=[
            pltpu.VMEM((fs_count, span, lanes), F32), pltpu.VMEM((fs_count, span, lanes), F32),
            pltpu.VMEM((fs_count, dspan, quarter), F32),
            pltpu.VMEM((fs_count, span, 2 * lanes), BF), pltpu.VMEM((fs_count, dspan, quarter), BF),
            pltpu.VMEM((16, wide), F32), pltpu.VMEM((full, 2 * lanes), BF), pltpu.VMEM((full, 2 * lanes), BF),
            pltpu.VMEM((held, lanes, quarter * cols), BF), pltpu.VMEM((lanes, quarter * cols), BF),
            pltpu.VMEM((full, lanes), BF), pltpu.VMEM((full, lanes), BF), dma(3), dma(8),
            pltpu.VMEM((cols, toks, quarter), BF), pltpu.VMEM((cols, toks, quarter), BF),
            pltpu.VMEM((chips, 2, rows, quarter), BF), pltpu.VMEM((wide, wide), BF),
            pltpu.VMEM((cols, held, slots, quarter), BF), pltpu.VMEM((chips, 2, 4 * SLOTS, wide), BF),
            pltpu.VMEM((dfull, quarter), BF), pltpu.VMEM((dfull, quarter), BF), pltpu.VMEM((dfull, quarter), BF),
            pltpu.VMEM((held, slots, lanes * cols), BF), pltpu.VMEM((toks, lanes * cols), BF),
            pltpu.VMEM((held, slots // parts, quarter), BF), pltpu.VMEM((chips, toks, quarter), F32),
            pltpu.VMEM((chips, toks, quarter), BF), pltpu.VMEM((chips, toks, quarter), BF), *ring,
            dma(chips, 2), dma(chips, 2), dma(chips, 2), dma(chips, 2), dma(chips), dma(chips), dma(chips), dma(chips),
            dma(4), dma(4), dma(2, 2, half), dma(2, 2, half), dma(chips, 2), dma(chips, 2),
            *[dma(chips)] * 6, *[dma(parts + 1)] * 6, dma(chips), dma(chips), dma(2, 2, half), dma(2, 2, half),
            dma(3, cols - 1), dma(3, cols - 1),
        ],
        compiler_params=pltpu.CompilerParams(collective_id=1, has_side_effects=True, vmem_limit_bytes=62 * 2**20),
        cost_estimate=pl.CostEstimate(flops=60_000_000_000, bytes_accessed=16_000_000, transcendentals=0),
    )(
        tokens, routes.T, route_weights.T, norm_gain.reshape(1, span), shared_gate, shared_up, shared_down,
        pairs_of(gate_experts), pairs_of(up_experts), pairs_of(down_experts),
    )
    return finish(mixed, gate_ready, up_ready, od, sg, su, os)


def solution(mesh):
    return jax.shard_map(
        per_device,
        mesh=mesh,
        in_specs=(
            P(("grp", "fs"), "tp"), P(("grp", "fs"), None), P(("grp", "fs"), None), P("fs"),
            P(None, "fs", "tp"), P(None, "fs", "tp"), P(None, "fs", "tp"),
            P("fs", "tp"), P("fs", "tp"), P("fs", "tp"),
        ),
        out_specs=(
            P(("grp", "fs"), "tp"), P(("grp", "fs"), None, "tp"), P(("grp", "fs"), None, "tp"),
            P(("grp", "fs"), "tp", None), P("grp", "tp"), P("grp", "tp"), P(("grp", "tp"), None),
        ),
        check_vma=False,
    )
```

```python
import functools

import jax
import jax.numpy as jnp
from jax import lax
from jax.experimental import pallas as pl
from jax.experimental.pallas import tpu as pltpu
from jax.sharding import PartitionSpec as P

MESH = pl.DeviceIdType.MESH
BF = jnp.bfloat16
F32 = jnp.float32
META = 16
SLOTS = 32


def remote(src, dst, send_sem, recv_sem, **where):
    return pltpu.make_async_remote_copy(
        src_ref=src, dst_ref=dst, send_sem=send_sem, recv_sem=recv_sem, device_id=where, device_id_type=MESH
    )


def far_first(count):
    half = count // 2
    order = [half]
    for d in range(1, half):
        order += [half - d, half + d]
    return order + [0]


def places(chips, cols):
    g, f, t = lax.axis_index("grp"), lax.axis_index("fs"), lax.axis_index("tp")
    c = lax.rem(f, 2)
    z = lax.div(f, 2)
    up = lax.rem(z + 1, chips) * 2 + c
    down = lax.rem(z + chips - 1, chips) * 2 + c
    other = f + 1 - 2 * c
    par = lax.rem(g, 2)
    pair = g + 1 - 2 * par
    right, left = lax.rem(t + 1, cols), lax.rem(t + cols - 1, cols)
    return f, t, c, z, up, down, other, par, pair, right, left


def greet(peers):
    barrier = pltpu.get_barrier_semaphore()
    for peer in peers:
        pl.semaphore_signal(barrier, inc=1, device_id=peer, device_id_type=MESH)

    def answered():
        pl.semaphore_wait(barrier, len(peers))

    return answered


def whole_kernel(
    chips, cols, held, top,
    tok, routes, weights_of, gain, sgate_own, sup_own, sdown_own, gates, ups, downs,
    mixed, gate_out, up_out, od_out, os_out, sg_out, su_out,
    gf, uf, df, gcast, dcast, table, gu, gu2, od, os, sg, su, in_sem, out_sem, raw, xn, buf, tri, x, gw, sd, dn, dn2, act, sact, y, own, ss, sr, ps, pr, ms, mr,
    gs, gr, ds_, dr, gys, gyr, dys, dyr, ts, tr, zs, zr, cs, cr, rs, rr, ls, lr, fs_, fr,
    ars, arr, als, alr, afs, afr, bs, br, vs, vr, ws, wr,
):
    f, t, c, z, up, down, other, par, pair, right, left = places(chips, cols)
    fs_count = 2 * chips
    half = chips // 2
    order = far_first(chips)
    pos = {r: p for p, r in enumerate(order)}
    toks, quarter = tok.shape
    lanes = sg.shape[1]
    rows = buf.shape[2]
    cut = rows // 2
    width = 2 * SLOTS
    wide = tri.shape[0]
    span, dspan = gcast.shape[1], dcast.shape[1]
    parts = 4
    per = chips // parts
    tall = per * width
    tcut = toks // 2
    across = [lax.rem(t + d, cols) for d in range(1, cols)]

    def core(delta, k):
        return lax.rem(z + delta, chips) * 2 + k

    away = [(delta, k) for delta in range(1, chips) for k in range(2)]
    fetched = [
        pltpu.make_async_copy(src.at[:, par], dst, in_sem.at[n])
        for n, (src, dst) in enumerate(((gates, gf), (ups, uf), (downs, df)))
    ]
    for copy in fetched:
        copy.start()
    answered = greet(
        [{"fs": core(delta, k)} for delta, k in away]
        + [{"fs": other}, {"grp": pair}]
        + [{"tp": a} for a in across]
    )
    sent = []

    def go(copy):
        copy.start()
        sent.append(copy)
        return copy

    def part(ref, owner, size, count=1):
        return ref.at[pl.ds(pl.multiple_of(owner * size, size), count * size), :]

    def hand(cast, target, size, sends, recvs, delta, k):
        there = core(delta, k)
        back = (chips - delta) % chips
        go(remote(cast.at[there], part(target, f, size), sends.at[delta, k], recvs.at[back, c], fs=there))

    def landed(target, size, sends, recvs, delta, k):
        here = part(target, core(delta, k), size)
        remote(here, here, sends.at[delta, k], recvs.at[delta, k], fs=core(delta, k)).wait_recv()

    def hand_gates(d):
        for delta in sorted({d, chips - d}):
            for k in range(2):
                hand(gcast, gu, span, gs, gr, delta, k)

    def swap_chip(target, target2, size, sends, recvs, delta):
        here, there = (part(v, core(delta, 0), size, 2) for v in (target, target2))
        return go(remote(here, there, sends.at[delta], recvs.at[delta], grp=pair))

    table[...] = jnp.full(table.shape, -1.0, F32)
    table[0:top, 0:toks] = routes[...].astype(F32)
    table[8 : 8 + top, 0:toks] = weights_of[...]
    turned = table[...]
    diagonal = lax.broadcasted_iota(jnp.int32, (span, span), 0) == lax.broadcasted_iota(jnp.int32, (span, span), 1)
    column = jnp.sum(jnp.where(diagonal, jnp.broadcast_to(gain[...], (span, span)), 0.0), axis=1, keepdims=True)
    weight = turned[8:16, :]
    high = weight.astype(BF)
    low = (weight - high.astype(F32)).astype(BF)
    short = span // 2
    scaled = [(v[...] * column).astype(BF) for v in (sgate_own, sup_own)]
    buf[0, c, toks : toks + 8, 0:wide] = turned[0:8, :].astype(BF)
    buf[0, c, toks : toks + 8, wide:] = high
    buf[0, c, toks + 8 : toks + META, 0:wide] = low
    buf[0, c, toks + 8 : toks + META, wide:] = jnp.zeros_like(low)
    for h in range(2):
        for n in range(2):
            at = (2 * h + n) * lanes
            buf[0, c, toks + META : toks + META + short, at : at + lanes] = scaled[n][h * short : (h + 1) * short]
    buf[0, c, toks + META + short :, :] = sdown_own[...].astype(BF)
    for copy in fetched:
        copy.wait()

    @pl.loop(0, fs_count)
    def _(i):
        gcast[i, :, 0:lanes] = (gf[i] * column).astype(BF)
        gcast[i, :, lanes:] = (uf[i] * column).astype(BF)
        dcast[i] = df[i].astype(BF)

    answered()
    traded = [
        go(remote(tok, raw.at[t], ts.at[0], tr.at[0], tp=right)),
        go(remote(tok, raw.at[t], ts.at[1], tr.at[1], tp=left)),
    ]
    for d in range(1, half // 2 + 1):
        hand_gates(d)
    go(remote(gcast.at[other], part(gu, f, span), gs.at[0, 0], gr.at[0, 0], fs=other))
    go(remote(dcast.at[other], part(dn, f, dspan), ds_.at[0, 0], dr.at[0, 0], fs=other))
    part(gu, f, span)[...] = gcast[f]
    part(dn, f, dspan)[...] = dcast[f]
    tri[...] = jnp.where(
        lax.broadcasted_iota(jnp.int32, (wide, wide), 0) < lax.broadcasted_iota(jnp.int32, (wide, wide), 1), 1.0, 0.0
    ).astype(BF)
    traded[0].wait_recv()
    upper, lower = pl.ds(0, tcut), pl.ds(tcut, tcut)
    traded.append(go(remote(raw.at[left, upper], raw.at[left, upper], ts.at[2], tr.at[2], tp=right)))
    traded[1].wait_recv()
    traded.append(go(remote(raw.at[right, lower], raw.at[right, lower], ts.at[3], tr.at[3], tp=left)))
    traded[2].wait_recv()
    traded[3].wait_recv()
    opposite = across[cols // 2 - 1]
    sources = [(t, tok)] + [(q, raw.at[q]) for q in (left, right, opposite)]
    total = jnp.zeros((toks, 1), F32)
    for _, ref in sources:
        value = ref[...].astype(F32)
        total += jnp.sum(value * value, axis=1, keepdims=True)
    scale = lax.rsqrt(total / (quarter * cols) + 1e-06)
    buf[0, c, 0:toks, :] = (tok[...].astype(F32) * scale).astype(BF)
    for q, ref in sources:
        xn[q] = (ref[...].astype(F32) * scale).astype(BF)

    def process(r):
        p = pos[r]

        @pl.loop(0, 2)
        def _(cc):
            meta = buf[r, cc, toks : toks + META, :].astype(F32)
            route, hi, lo = meta[0:8, 0:wide], meta[0:8, wide:], meta[8:META, 0:wide]
            named, his, los = [], [], []
            for j in range(held):
                hit = route == (f * held + j).astype(F32)
                named.append(jnp.sum(jnp.where(hit, 1.0, 0.0), axis=0, keepdims=True))
                his.append(jnp.sum(jnp.where(hit, hi, 0.0), axis=0, keepdims=True))
                los.append(jnp.sum(jnp.where(hit, lo, 0.0), axis=0, keepdims=True))
            stack = jnp.concatenate(named + [jnp.zeros((8 - held, wide), F32)], axis=0)
            rank = jnp.dot(stack.astype(BF), tri[...], preferred_element_type=F32)
            slot = lax.broadcasted_iota(jnp.int32, (SLOTS, wide), 0).astype(F32)
            picks, ghi, glo = [], [], []
            for j in range(held):
                pick = jnp.where(slot == rank[j : j + 1], 1.0, 0.0) * named[j]
                picks.append(pick)
                ghi.append(pick * his[j])
                glo.append(pick * los[j])
            chosen = jnp.concatenate(picks, axis=0).astype(BF)
            gw[p, cc] = jnp.concatenate(ghi + glo, axis=0).astype(BF)
            got = jnp.dot(chosen, buf[r, cc, 0:wide, :], preferred_element_type=F32).astype(BF)
            at = pl.multiple_of(p * width + cc * SLOTS, SLOTS)
            for j in range(held):
                x[t, j, pl.ds(at, SLOTS), :] = got[j * SLOTS : (j + 1) * SLOTS]
            owner = lax.rem(z + r, chips) * 2 + cc
            piece = buf[r, cc, toks + META : toks + META + short, :]
            for h in range(2):
                there = pl.ds(pl.multiple_of(owner * span + h * short, short), short)
                sg[there, :] = piece[:, 2 * h * lanes : (2 * h + 1) * lanes]
                su[there, :] = piece[:, (2 * h + 1) * lanes : (2 * h + 2) * lanes]
            sd[pl.ds(pl.multiple_of(owner * dspan, dspan), dspan), :] = buf[r, cc, toks + META + short :, :]

    def block(q, p):
        return x.at[q, :, pl.ds(p * width, width), :]

    to_right, to_left, onward = {}, {}, {}

    def send_rows(r):
        p = pos[r]
        to_right[p] = go(remote(block(t, p), block(t, p), rs.at[p], rr.at[p], tp=right))
        to_left[p] = go(remote(block(t, p), block(t, p), ls.at[p], lr.at[p], tp=left))

    def pass_rows(p):
        to_right[p].wait_recv()
        to_left[p].wait_recv()
        source, target = (left, right) if p % 2 == 0 else (right, left)
        onward[p] = go(remote(block(source, p), block(source, p), fs_.at[p], fr.at[p], tp=target))

    ring, sib = {}, {}
    bounds = [pl.ds(0, cut), pl.ds(cut, cut)]

    def forward(way, h, d):
        step = chips - d if way == 0 else d
        before = (step + 1) % chips if way == 0 else step - 1
        src, dst = buf.at[before, c, bounds[h]], buf.at[step, c, bounds[h]]
        ring[way, h, d] = go(
            remote(src, dst, zs.at[way, h, d - 1], zr.at[way, h, d - 1], fs=up if way == 0 else down)
        )

    def share(r, h):
        here = buf.at[r, c, bounds[h]]
        sib[r, h] = go(remote(here, here, cs.at[r, h], cr.at[r, h], fs=other))

    flows = [(0, 0), (1, 1), (0, 1), (1, 0)]
    for way, h in flows:
        forward(way, h, 1)
    for h in range(2):
        share(0, h)
    waiting = []
    gate_swaps = {}

    def swap_gates(delta):
        for k in range(2):
            landed(gu, span, gs, gr, delta, k)
        gate_swaps[delta] = swap_chip(gu, gu2, span, gys, gyr, delta)

    remote(part(gu, other, span), part(gu, other, span), gs.at[0, 0], gr.at[0, 0], fs=other).wait_recv()
    gate_swaps[0] = swap_chip(gu, gu2, span, gys, gyr, 0)

    def settle(near):
        for r in near:
            for h in range(2):
                sib[r, h].wait_recv()
            process(r)
        for r in near:
            send_rows(r)
        waiting.extend(pos[r] for r in near)

    def swap_ring(d):
        for delta in sorted({d, chips - d}):
            swap_gates(delta)

    def pass_waiting():
        while waiting:
            pass_rows(waiting.pop(0))

    ready = {half // 2: (1,), half // 2 + 1: (2, 3), half - 2: (4,), half - 1: (5,), half: (6,)} if half == 8 else {}

    def hand_downs():
        for d in range(half, 0, -1):
            for delta in sorted({d, chips - d}):
                for k in range(2):
                    hand(dcast, dn, dspan, ds_, dr, delta, k)

    settle([0])
    for d in range(1, half + 1):
        for way, h in flows:
            if d == half and way != h:
                continue
            ring[way, h, d].wait_recv()
            if d + 1 < half or (d + 1 == half and way == h):
                forward(way, h, d + 1)
            share(chips - d if way == 0 else d, h)
        later = half // 2 + (d + 1) // 2
        if d % 2 == 1 and later <= half:
            hand_gates(later)
        if d == half - 1:
            hand_downs()
        if d < half:
            pass_waiting()
            settle([chips - d, d])
        else:
            settle([half])
        for n in ready.get(d, ()):
            swap_ring(n)
    onward[pos[half]] = go(
        remote(block(t, pos[half]), block(t, pos[half]), fs_.at[pos[half]], fr.at[pos[half]], tp=opposite)
    )
    waiting.remove(pos[half])
    pass_waiting()
    for n in range(1, half + 1):
        if n not in sum(ready.values(), ()):
            swap_ring(n)
    down_swaps = []

    def land_downs(d):
        d = half + 1 - d if d else 0
        for delta in sorted({d, chips - d} if d else {0}):
            if delta:
                for k in range(2):
                    landed(dn, dspan, ds_, dr, delta, k)
            else:
                remote(part(dn, other, dspan), part(dn, other, dspan), ds_.at[0, 0], dr.at[0, 0], fs=other).wait_recv()
            down_swaps.append(swap_chip(dn, dn2, dspan, dys, dyr, delta))

    for d in range(3):
        land_downs(d)
    to_right[pos[half]].wait_recv()
    to_left[pos[half]].wait_recv()
    for p in onward:
        onward[p].wait_recv()
    for d in range(3, half // 2 + 1):
        land_downs(d)

    own_lanes = pl.ds(pl.multiple_of(t * lanes, lanes), lanes)

    def hidden(j, at, weights):
        both = jnp.zeros((tall, 2 * lanes), F32)
        for q in range(cols):
            both += jnp.dot(x[q, j, at, :], weights[q * quarter : (q + 1) * quarter, :], preferred_element_type=F32)
        act[j, at, own_lanes] = (jax.nn.silu(both[:, :lanes]) * both[:, lanes:]).astype(BF)

    @pl.loop(0, parts)
    def _(i):
        hidden(par, pl.ds(pl.multiple_of(i * tall, tall), tall), gu)

    for delta in gate_swaps:
        gate_swaps[delta].wait_recv()
    land_downs(half // 2 + 1)
    outs = []

    def leave(src, dst):
        copy = pltpu.make_async_copy(src, dst, out_sem.at[len(outs)])
        copy.start()
        outs.append(copy)

    to_right2, to_left2, onward2 = {}, {}, {}

    def piece(q, i):
        cols_of = pl.ds(pl.multiple_of(q * lanes, lanes), lanes)
        return sact.at[:, cols_of] if i == parts else act.at[:, pl.ds(i * tall, tall), cols_of]

    def send_act(i):
        to_right2[i] = go(remote(piece(t, i), piece(t, i), ars.at[i], arr.at[i], tp=right))
        to_left2[i] = go(remote(piece(t, i), piece(t, i), als.at[i], alr.at[i], tp=left))

    def pass_act(i):
        to_right2[i].wait_recv()
        to_left2[i].wait_recv()
        if i == 0:
            return
        source, target = (left, right) if i % 2 == 0 else (right, left)
        onward2[i] = go(remote(piece(source, i), piece(source, i), afs.at[i], afr.at[i], tp=target))

    for i in range(parts):
        hidden(1 - par, pl.ds(i * tall, tall), gu2)
        send_act(i)
        if i == 0:
            onward2[0] = go(remote(piece(t, 0), piece(t, 0), afs.at[0], afr.at[0], tp=opposite))
    sgate = jnp.zeros((toks, lanes), F32)
    sup = jnp.zeros((toks, lanes), F32)
    for q in range(cols):
        there = slice(q * quarter, (q + 1) * quarter)
        sgate += jnp.dot(xn[q], sg[there, :], preferred_element_type=F32)
        sup += jnp.dot(xn[q], su[there, :], preferred_element_type=F32)
    sact[:, own_lanes] = (jax.nn.silu(sgate) * sup).astype(BF)
    send_act(parts)
    placed = []

    def place(kind, source, target):
        home = pl.ds(pl.multiple_of(t * quarter, quarter), quarter)
        for k, a in enumerate(across):
            rows_of = pl.ds(pl.multiple_of(a * lanes, lanes), lanes)
            placed.append(go(remote(source.at[rows_of, :], target.at[:, home], ws.at[kind, k], wr.at[kind, k], tp=a)))
        target[:, home] = source[pl.ds(pl.multiple_of(t * lanes, lanes), lanes), :]

    for d in range(half // 2 + 2, half + 1):
        land_downs(d)
    pass_act(0)
    for copy in down_swaps:
        copy.wait_recv()
    sibs = {}

    def chunk(i):
        onward2[i].wait_recv()
        for j, weights in ((par, dn), (1 - par, dn2)):
            y[j] = jnp.dot(act[j, i * tall : (i + 1) * tall, :], weights[...], preferred_element_type=F32).astype(BF)

        def combine(p, u, cc):
            at = pl.ds(pl.multiple_of(u * width + cc * SLOTS, SLOTS), SLOTS)
            found = jnp.concatenate([y[0, at, :], y[1, at, :]], axis=0)
            twice = jnp.concatenate([found, found], axis=0)
            whole = lax.dot_general(gw[p, cc], twice, (((0,), (0,)), ((), ())), preferred_element_type=F32)
            return whole[0:toks]

        for u in range(per):
            p = i * per + u
            ss[p] = combine(p, u, 1 - c).astype(BF)
            sibs[p] = go(remote(ss.at[p], sr.at[p], bs.at[p], br.at[p], fs=other))
            own[p] = combine(p, u, c)
            if p == 1:
                step(0)

    sums = {}
    limits = [slice(0, tcut), slice(tcut, toks)]
    met = set()

    def local(r, h):
        p = pos[r]
        if p not in met:
            met.add(p)
            sibs[p].wait_recv()
        return own[p, limits[h], :] + sr[p, limits[h], :].astype(F32)

    def add_on(way, h, r):
        out, into = ((ps, pr), (ms, mr))[way]
        k = half - r if way == 0 else r - half
        value = local(r, h)
        first = way != h and k == 1 or k == 0
        if not first:
            sums[way, h, k - 1].wait_recv()
            value = value + into[k - 1, limits[h], :].astype(F32)
        out[k, limits[h], :] = value.astype(BF)
        there = (upper, lower)[h]
        sums[way, h, k] = go(
            remote(out.at[k, there], into.at[k, there], vs.at[way, h, k], vr.at[way, h, k], fs=up if way == 0 else down)
        )

    def step(k):
        for way, h in flows:
            if k == 0 and way != h:
                continue
            add_on(way, h, half - k if way == 0 else half + k)

    done = 1
    for i in range(parts):
        chunk(i)
        if i == 0:
            pass_act(1)
            pass_act(2)
        while done < half and max(pos[half - done], pos[(half + done) % chips]) < (i + 1) * per and done <= 2 * i:
            step(done)
            done += 1
        if i == 0:
            place(0, dn, od.at[par])
            place(1, dn2, od.at[1 - par])
            place(2, sd, os)
            for n, (mine, theirs, target) in enumerate(
                ((gu, gu2, gate_out), (gu, gu2, up_out))
            ):
                these = pl.ds(n * lanes, lanes)
                leave(mine.at[:, these], target.at[par])
                leave(theirs.at[:, these], target.at[1 - par])
            pass_act(3)
            pass_act(4)
            leave(sg, sg_out)
            leave(su, su_out)
    onward2[parts].wait_recv()
    shared = jnp.dot(sact[...], sd[...], preferred_element_type=F32)
    own[pos[0]] = own[pos[0]] + shared
    while done < half:
        step(done)
        done += 1
    for copy in placed:
        copy.wait_recv()
    leave(od, od_out)
    leave(os, os_out)
    for h in range(2):
        value = local(0, h)
        for way in range(2):
            sums[way, h, half - 1].wait_recv()
            value = value + (pr, mr)[way][half - 1, limits[h], :].astype(F32)
        mixed[limits[h], :] = value.astype(BF)
    for copy in outs:
        copy.wait()
    for copy in sent:
        copy.wait_send()


VM = pl.BlockSpec(memory_space=pltpu.VMEM)
ANY = pl.BlockSpec(memory_space=pl.ANY)


def shape(*dims, kind=BF):
    return jax.ShapeDtypeStruct(dims, kind)


def finish_kernel(count, *refs):
    ins, outs, bufs = refs[:count], refs[count : 2 * count], refs[2 * count : 3 * count]
    in_sem, out_sem = refs[3 * count :]
    reads = [pltpu.make_async_copy(ins[n], bufs[n], in_sem.at[n]) for n in range(count)]
    writes = [pltpu.make_async_copy(bufs[n], outs[n], out_sem.at[n]) for n in range(count)]
    for copy in reads:
        copy.start()
    for n in range(count):
        reads[n].wait()
        writes[n].start()
    for copy in writes:
        copy.wait()


def finish(*arrays):
    count = len(arrays)
    sems = [pltpu.SemaphoreType.DMA((count,))] * 2
    return pl.pallas_call(
        functools.partial(finish_kernel, count),
        out_shape=tuple(shape(*a.shape, kind=a.dtype) for a in arrays),
        in_specs=[ANY] * count,
        out_specs=(ANY,) * count,
        scratch_shapes=[pltpu.VMEM(a.shape, a.dtype) for a in arrays] + sems,
    )(*arrays)


def per_device(
    tokens, routes, route_weights, norm_gain, gate_experts, up_experts, down_experts, shared_gate, shared_up, shared_down
):
    fs_count, cols = lax.axis_size("fs"), lax.axis_size("tp")
    chips = fs_count // 2
    experts, span, lanes = gate_experts.shape
    held = experts // fs_count
    toks, quarter = tokens.shape
    top = routes.shape[1]
    dspan = down_experts.shape[1]
    wide = quarter // 2

    def pairs_of(w):
        return w.reshape(fs_count, held, *w.shape[1:])

    def dma(*dims):
        return pltpu.SemaphoreType.DMA(dims)

    slots = chips * 2 * SLOTS
    half = chips // 2
    parts = 4
    rows = toks + META + span // 2 + dspan
    full, dfull = fs_count * span, fs_count * dspan
    ring = [pltpu.VMEM((half, toks, quarter), BF)] * 4
    mixed, gate_ready, up_ready, od, os, sg, su = pl.pallas_call(
        functools.partial(whole_kernel, chips, cols, held, top),
        out_shape=(
            shape(toks, quarter), shape(held, full, lanes), shape(held, full, lanes), shape(held, lanes, quarter * cols),
            shape(lanes, quarter * cols), shape(full, lanes), shape(full, lanes),
        ),
        in_specs=[VM] * 7 + [ANY] * 3,
        out_specs=(VM,) + (ANY,) * 6,
        scratch_shapes=[
            pltpu.VMEM((fs_count, span, lanes), F32), pltpu.VMEM((fs_count, span, lanes), F32),
            pltpu.VMEM((fs_count, dspan, quarter), F32),
            pltpu.VMEM((fs_count, span, 2 * lanes), BF), pltpu.VMEM((fs_count, dspan, quarter), BF),
            pltpu.VMEM((16, wide), F32), pltpu.VMEM((full, 2 * lanes), BF), pltpu.VMEM((full, 2 * lanes), BF),
            pltpu.VMEM((held, lanes, quarter * cols), BF), pltpu.VMEM((lanes, quarter * cols), BF),
            pltpu.VMEM((full, lanes), BF), pltpu.VMEM((full, lanes), BF), dma(3), dma(8),
            pltpu.VMEM((cols, toks, quarter), BF), pltpu.VMEM((cols, toks, quarter), BF),
            pltpu.VMEM((chips, 2, rows, quarter), BF), pltpu.VMEM((wide, wide), BF),
            pltpu.VMEM((cols, held, slots, quarter), BF), pltpu.VMEM((chips, 2, 4 * SLOTS, wide), BF),
            pltpu.VMEM((dfull, quarter), BF), pltpu.VMEM((dfull, quarter), BF), pltpu.VMEM((dfull, quarter), BF),
            pltpu.VMEM((held, slots, lanes * cols), BF), pltpu.VMEM((toks, lanes * cols), BF),
            pltpu.VMEM((held, slots // parts, quarter), BF), pltpu.VMEM((chips, toks, quarter), F32),
            pltpu.VMEM((chips, toks, quarter), BF), pltpu.VMEM((chips, toks, quarter), BF), *ring,
            dma(chips, 2), dma(chips, 2), dma(chips, 2), dma(chips, 2), dma(chips), dma(chips), dma(chips), dma(chips),
            dma(4), dma(4), dma(2, 2, half), dma(2, 2, half), dma(chips, 2), dma(chips, 2),
            *[dma(chips)] * 6, *[dma(parts + 1)] * 6, dma(chips), dma(chips), dma(2, 2, half), dma(2, 2, half),
            dma(3, cols - 1), dma(3, cols - 1),
        ],
        compiler_params=pltpu.CompilerParams(collective_id=1, has_side_effects=True, vmem_limit_bytes=62 * 2**20),
        cost_estimate=pl.CostEstimate(flops=60_000_000_000, bytes_accessed=16_000_000, transcendentals=0),
    )(
        tokens, routes.T, route_weights.T, norm_gain.reshape(1, span), shared_gate, shared_up, shared_down,
        pairs_of(gate_experts), pairs_of(up_experts), pairs_of(down_experts),
    )
    return finish(mixed, gate_ready, up_ready, od, sg, su, os)


def solution(mesh):
    return jax.shard_map(
        per_device,
        mesh=mesh,
        in_specs=(
            P(("grp", "fs"), "tp"), P(("grp", "fs"), None), P(("grp", "fs"), None), P("fs"),
            P(None, "fs", "tp"), P(None, "fs", "tp"), P(None, "fs", "tp"),
            P("fs", "tp"), P("fs", "tp"), P("fs", "tp"),
        ),
        out_specs=(
            P(("grp", "fs"), "tp"), P(("grp", "fs"), None, "tp"), P(("grp", "fs"), None, "tp"),
            P(("grp", "fs"), "tp", None), P("grp", "tp"), P("grp", "tp"), P(("grp", "tp"), None),
        ),
        check_vma=False,
    )
```
